32 devices in a mesh: grp: 2 (over y), fs: 4 (over z), tp: 4 (over x, core).
Axes of the slice: x: 2, y: 2, z: 4, core: 2. Of those that a mesh axis runs over, the one named last changes fastest.
Arguments:
- tokens: bfloat16 [2048, 2048], P(('grp', 'fs', 'tp')), parts along dimension 0, may hold values from -30 to 30
- gate_master: float32 [2048, 2752], P('fs', 'tp'), may hold values from -0.125 to 0.125
- up_master: float32 [2048, 2752], P('fs', 'tp'), may hold values from -0.125 to 0.125
- down_master: float32 [2048, 2752], P('fs', 'tp'), may hold values from -0.4375 to 0.4375
- norm_gain: float32 [2048], replicated, may hold values from 0.1 to 1.9
- post_gain: float32 [2048], replicated, may hold values from 0.1 to 1.9
- post_bias: float32 [2048], replicated, may hold values from -3 to 3
Outputs:
- gate_ready: bfloat16 [4096, 2752], P('grp', 'tp'), parts along dimension 0
- up_ready: bfloat16 [4096, 2752], P('grp', 'tp'), parts along dimension 0
- down_ready: bfloat16 [4096, 2752], P('grp', 'tp'), parts along dimension 0
- result: bfloat16 [2048, 2048], P(('grp', 'fs', 'tp')), parts along dimension 0
The draws below stay inside these ranges and needn't reach their ends.
There are 2 independent parts, one for each index of `grp`. The reference program is written for one: setup_inputs(seed, part) draws one part's arguments, and reference() takes and returns one part's arrays. A program takes and returns all parts, laid end to end along the dimension named above; an argument that names none is the same for every part. Nothing has to cross between parts.
All inputs are finite; a program needn't handle non-finite values.
Results may differ from the reference program's by a relative error of at most 0.009.
Values may be sent and summed in bfloat16 or wider, within the bound.
A program may use at most 64 MiB of HBM per device.

```python
import math
import jax
import jax.numpy as jnp
from jax import lax

D = 2048
FF = 2752
TOKENS = 1024
N_TP = 4


def draw_tokens(key, part):
    key_base, key_rows, key_cols = jax.random.split(key, 3)
    row_scale = jnp.exp(jax.random.uniform(key_rows, (TOKENS, 1), jnp.float32, math.log(0.3), math.log(3.0)))
    col_scale = jnp.exp(jax.random.uniform(key_cols, (1, D), jnp.float32, math.log(0.5), math.log(2.0)))
    base = jnp.clip(jax.random.normal(key_base, (TOKENS, D), jnp.float32), -4.0, 4.0)
    return (base * row_scale * col_scale).astype(jnp.bfloat16)


def shard_levels(rng, dims, pieces, least, top_value):
    gain = 1.0
    for axis_at, parts in pieces:
        draws = jax.random.uniform(jax.random.fold_in(jax.random.fold_in(rng, 6), axis_at), (parts,), jnp.float32, least / len(pieces), top_value / len(pieces))
        gain = gain * jnp.repeat(jnp.exp(draws), dims[axis_at] // parts).reshape((-1,) + (1,) * (len(dims) - 1 - axis_at))
    return gain


def centred(key, shape, deviation, most, cuts=(), kind=jnp.bfloat16):
    values = deviation * jax.random.normal(key, shape, jnp.float32)
    if cuts:
        values = values * shard_levels(key, shape, cuts, -0.22, 0.18)
    return jnp.clip(values, -most, most).astype(kind)


def setup_inputs(seed: int = 0, part: int = 0) -> dict:
    streams_of = jax.random.split(jax.random.key(seed), 8)
    part_keys = jax.random.split(jax.random.fold_in(streams_of[7], part), 8)
    return {
        "tokens": draw_tokens(jax.random.fold_in(jax.random.fold_in(streams_of[7], part), 71), part),
        "gate_master": centred(streams_of[1], (D, FF), D ** -0.5, 0.125, ((0, 4), (1, 4)), jnp.float32),
        "up_master": centred(streams_of[2], (D, FF), D ** -0.5, 0.125, ((0, 4), (1, 4)), jnp.float32),
        "down_master": centred(streams_of[3], (D, FF), (FF // 16) ** -0.5, 0.4375, ((0, 4), (1, 4)), jnp.float32),
        "norm_gain": jnp.clip(1.0 + 0.18 * jax.random.normal(streams_of[4], (D,), jnp.float32), 0.1, 1.9),
        "post_gain": jnp.clip(1.0 + 0.18 * jax.random.normal(streams_of[5], (D,), jnp.float32), 0.1, 1.9),
        "post_bias": centred(streams_of[6], (D,), 0.5, 3.0, (), jnp.float32),
    }


def reference(tokens, gate_master, up_master, down_master, norm_gain, post_gain, post_bias):
    gate_ready = (norm_gain[:, None] * gate_master).astype(jnp.bfloat16)
    up_ready = (norm_gain[:, None] * up_master).astype(jnp.bfloat16)
    down_ready = down_master.astype(jnp.bfloat16)
    wide = tokens.astype(jnp.float32)
    normed = (wide * lax.rsqrt(lax.optimization_barrier(jnp.mean(wide * wide, axis=-1, keepdims=True)) + 1e-06)).astype(jnp.bfloat16)
    gate = jnp.dot(normed, gate_ready, preferred_element_type=jnp.float32)
    upward = jnp.dot(normed, up_ready, preferred_element_type=jnp.float32)
    hidden = (jax.nn.silu(gate) * upward).astype(jnp.bfloat16)
    block_units = FF // N_TP
    branch = jnp.zeros((tokens.shape[0], D), jnp.float32)
    for block in range(N_TP):
        part_hidden = hidden[:, block * block_units:(block + 1) * block_units]
        part_down = down_ready[:, block * block_units:(block + 1) * block_units]
        partial_value = lax.dot_general(part_hidden, part_down, (((1,), (1,)), ((), ())), preferred_element_type=jnp.float32)
        rounded = lax.optimization_barrier(partial_value.astype(jnp.bfloat16))
        branch = branch + rounded.astype(jnp.float32)
    mixed = jnp.sqrt(jnp.float32(2.0)) * wide + 0.5 * branch
    center = lax.optimization_barrier(jnp.mean(mixed, axis=-1, keepdims=True))
    spread = lax.optimization_barrier(jnp.mean(jnp.square(mixed - center), axis=-1, keepdims=True))
    result = ((mixed - center) * lax.rsqrt(spread + 1e-05) * post_gain + post_bias).astype(jnp.bfloat16)
    return (gate_ready, up_ready, down_ready, result)
```

```python
import functools

import jax
import jax.numpy as jnp
from jax import lax
from jax.experimental import pallas as pl
from jax.experimental.pallas import tpu as pltpu
from jax.sharding import PartitionSpec as P

MESH = pl.DeviceIdType.MESH
LANES = 128


def finish(wide, branch, post_gain, post_bias):
    mixed = jnp.sqrt(jnp.float32(2.0)) * wide + 0.5 * branch
    center = jnp.mean(mixed, axis=-1, keepdims=True)
    spread = jnp.mean(jnp.square(mixed - center), axis=-1, keepdims=True)
    return ((mixed - center) * lax.rsqrt(spread + 1e-05) * post_gain + post_bias).astype(
        jnp.bfloat16
    )


def plain(tokens, gate_master, up_master, down_master, norm_gain, post_gain, post_bias):
    row_count = gate_master.shape[0]
    first_row = lax.axis_index("fs") * row_count
    gain_rows = lax.dynamic_slice_in_dim(norm_gain, first_row, row_count, 0)
    gate_piece = (gain_rows[:, None] * gate_master).astype(jnp.bfloat16)
    up_piece = (gain_rows[:, None] * up_master).astype(jnp.bfloat16)
    down_piece = down_master.astype(jnp.bfloat16)
    gate_ready, up_ready, down_ready = (
        lax.all_gather(gate_piece, "fs", axis=0, tiled=True),
        lax.all_gather(up_piece, "fs", axis=0, tiled=True),
        lax.all_gather(down_piece, "fs", axis=0, tiled=True),
    )
    wide = tokens.astype(jnp.float32)
    normed = (wide * lax.rsqrt(jnp.mean(wide * wide, axis=-1, keepdims=True) + 1e-06)).astype(
        jnp.bfloat16
    )
    piece = lax.all_gather(normed, "tp", axis=0, tiled=True)
    gate = jnp.dot(piece, gate_ready, preferred_element_type=jnp.float32)
    upward = jnp.dot(piece, up_ready, preferred_element_type=jnp.float32)
    hidden = (jax.nn.silu(gate) * upward).astype(jnp.bfloat16)
    branch = lax.psum_scatter(
        lax.dot_general(
            hidden, down_ready, (((1,), (1,)), ((), ())), preferred_element_type=jnp.float32
        ).astype(jnp.bfloat16),
        "tp",
        scatter_dimension=0,
        tiled=True,
    ).astype(jnp.float32)
    result = finish(wide, branch, post_gain, post_bias)
    return (gate_ready, up_ready, down_ready, result)


def fused_kernel(
    fs, tp, n, tok_ref, gm_ref, um_ref, dm_ref, gain_ref,
    fg, fu, fd, mixed,
    stage, toks, acc_g, acc_u, hid, parts, got,
    up_sem, dn_sem, y_sem, r_sem, ts_sem, tr_sem, ps_sem, pr_sem, i_sem,
):
    y, z, t = lax.axis_index("grp"), lax.axis_index("fs"), lax.axis_index("tp")
    cols, rc = gm_ref.shape
    tok_rows, d = tok_ref.shape
    tiles = d // LANES
    full = (fg, fu, fd)
    masters = (gm_ref, um_ref, dm_ref)
    up_dev = (y, jnp.minimum(z + 1, fs - 1), t)
    dn_dev = (y, jnp.maximum(z - 1, 0), t)
    y_dev = (1 - y, z, t)
    has_up, has_dn = z < fs - 1, z > 0
    peers = [lax.rem(t + j, tp) for j in range(1, tp)]
    first = [(m, c) for m in (0, 1) for c in range(n)]
    second = [(2, c) for c in range(n)]

    def fetch(m, h, c):
        k = h * n + c
        return pltpu.make_async_copy(
            masters[m].at[:, pl.ds(pl.multiple_of(k * LANES, LANES), LANES)],
            stage.at[m, k], i_sem.at[m, k],
        )

    for h in (y, 1 - y):
        for m, c in first + second:
            fetch(m, h, c).start()

    barrier = pltpu.get_barrier_semaphore()

    def greet(dev):
        pl.semaphore_signal(barrier, inc=1, device_id=dev, device_id_type=MESH)

    pl.when(has_up)(lambda: greet(up_dev))
    pl.when(has_dn)(lambda: greet(dn_dev))
    greet(y_dev)
    for peer in peers:
        greet((y, z, peer))

    def tile_of(b, h, c):
        return b * (2 * n) + h * n + c

    def hop(m, k, dev, sem):
        s = m * tiles + k
        return pltpu.make_async_remote_copy(
            src_ref=full[m].at[k], dst_ref=full[m].at[k], send_sem=sem.at[s], recv_sem=r_sem.at[s],
            device_id=dev, device_id_type=MESH,
        )

    def keep(m, h, c):
        fetch(m, h, c).wait()
        k = tile_of(z, h, c)
        v = stage[m, h * n + c]
        if m < 2:
            v = v * gain_ref[:, pl.ds(pl.multiple_of(k * LANES, LANES), LANES)]
        full[m][k] = v.astype(jnp.bfloat16)

    def send_own(m, c):
        k = tile_of(z, y, c)
        pl.when(has_up)(lambda: hop(m, k, up_dev, up_sem).start())
        pl.when(has_dn)(lambda: hop(m, k, dn_dev, dn_sem).start())

    def part_copy(k, j, peer):
        return pltpu.make_async_remote_copy(
            src_ref=parts.at[k, pl.ds(pl.multiple_of(peer * tok_rows, tok_rows), tok_rows)],
            dst_ref=got.at[t, k],
            send_sem=ps_sem.at[j, k], recv_sem=pr_sem.at[t, k],
            device_id=(y, z, peer), device_id_type=MESH,
        )

    def down_tile(k):
        part = jnp.dot(hid[...], fd[k], preferred_element_type=jnp.float32)
        parts[k] = part.astype(jnp.bfloat16)
        for j, peer in enumerate(peers):
            part_copy(k, j, peer).start()

    def add_tiles(m, k, start):
        acc = (acc_g, acc_u)[m]
        at = pl.ds(pl.multiple_of(k * LANES, LANES), n * LANES)
        lhs = toks[:, :, at].reshape(tp * tok_rows, n * LANES)
        rhs = jnp.concatenate([full[m][k + i] for i in range(n)], axis=1)
        term = lax.dot_general(
            lhs, rhs, (((1,), (1,)), ((), ())), preferred_element_type=jnp.float32
        )
        acc[...] = term if start else acc[...] + term

    def ends(p):
        low, high = z - 1 - p, z + 1 + p
        return ((low, low >= 0), (high, high <= fs - 1))

    sums, downs = [], []

    def later(m, b, ok, h, c):
        if m == 2:
            downs.append((ok, lambda: down_tile(tile_of(b, h, c))))
        elif c == n - 1:
            sums.append((ok, lambda: add_tiles(m, tile_of(b, h, 0), False)))

    def work(todo, count):
        for _ in range(min(count, len(todo))):
            ok, item = todo.pop(0)
            if ok is None:
                item()
            else:
                pl.when(ok)(item)

    def arrived(m, c, p):
        (low, has_low), (high, has_high) = ends(p)

        @pl.when(has_low)
        def _():
            k = tile_of(low, y, c)
            hop(m, k, up_dev, up_sem).wait_recv()
            hop(m, k, y_dev, y_sem).start()
            pl.when(has_up)(lambda: hop(m, k, up_dev, up_sem).start())

        @pl.when(has_high)
        def _():
            k = tile_of(high, y, c)
            hop(m, k, dn_dev, dn_sem).wait_recv()
            hop(m, k, y_dev, y_sem).start()
            pl.when(has_dn)(lambda: hop(m, k, dn_dev, dn_sem).start())

        for b, ok in ends(p):
            later(m, b, ok, y, c)

    def crossed(m, c, p):
        for b, ok in ends(p):
            @pl.when(ok)
            def _(b=b):
                k = tile_of(b, 1 - y, c)
                hop(m, k, y_dev, y_sem).wait_recv()
            later(m, b, ok, 1 - y, c)

    def tok_copy(j, peer, origin):
        return pltpu.make_async_remote_copy(
            src_ref=toks.at[origin], dst_ref=toks.at[origin],
            send_sem=ts_sem.at[j], recv_sem=tr_sem.at[origin],
            device_id=(y, z, peer), device_id_type=MESH,
        )

    wide = tok_ref[...].astype(jnp.float32)
    scale = lax.rsqrt(jnp.mean(wide * wide, axis=-1, keepdims=True) + 1e-06)
    toks[t] = (wide * scale).astype(jnp.bfloat16)
    keep(first[0][0], y, first[0][1])
    expected = has_up.astype(jnp.int32) + has_dn.astype(jnp.int32) + tp
    pl.semaphore_wait(barrier, expected)
    for before, pair in zip(first, first[1:]):
        keep(pair[0], y, pair[1])
        send_own(*before)
    for m, c in second:
        keep(m, y, c)
    send_own(*first[-1])
    for j, peer in enumerate(peers):
        tok_copy(j, peer, t).start()
    for m, c in first + second:
        keep(m, 1 - y, c)
    waiting = []
    for p in range(fs - 1):
        for m, c in first:
            arrived(m, c, p)
            waiting.append((m, c, p))
            if len(waiting) > 2 * len(first):
                crossed(*waiting.pop(0))
            if p > 0:
                work(sums, 4)
        if p == 0:
            for j, peer in enumerate(peers):
                tok_copy(j, peer, peer).wait_recv()
            own = [
                (None, lambda m=m, h=h: add_tiles(m, tile_of(z, h, 0), h == 0))
                for m in (0, 1) for h in (0, 1)
            ]
            sums[:0] = own
    for pair in second:
        send_own(*pair)
    for p in range(fs - 1):
        for m, c in second:
            arrived(m, c, p)
            waiting.append((m, c, p))
            if p > 0 and len(waiting) > 2:
                crossed(*waiting.pop(0))
            work(downs if p > 0 else sums, 4)
        if p == 0:
            while waiting[0][0] < 2:
                crossed(*waiting.pop(0))
            work(sums, len(sums))
            hid[...] = (jax.nn.silu(acc_g[...]) * acc_u[...]).astype(jnp.bfloat16)
            downs[:0] = [
                (None, lambda h=h, c=c: down_tile(tile_of(z, h, c)))
                for h in (0, 1) for c in range(n)
            ]
    while waiting:
        crossed(*waiting.pop(0))
    work(downs, len(downs))

    wide = tok_ref[...].astype(jnp.float32)
    mine = pl.ds(pl.multiple_of(t * tok_rows, tok_rows), tok_rows)
    for k in range(tiles):
        branch = parts[k, mine, :].astype(jnp.float32)
        for j, peer in enumerate(peers):
            pltpu.make_async_remote_copy(
                src_ref=got.at[peer, k], dst_ref=got.at[peer, k],
                send_sem=ps_sem.at[j, k], recv_sem=pr_sem.at[peer, k],
                device_id=(y, z, peer), device_id_type=MESH,
            ).wait_recv()
            branch = branch + got[peer, k].astype(jnp.float32)
        at = slice(k * LANES, (k + 1) * LANES)
        mixed[:, at] = jnp.sqrt(jnp.float32(2.0)) * wide[:, at] + 0.5 * branch

    for j, peer in enumerate(peers):
        tok_copy(j, peer, t).wait_send()
        for k in range(tiles):
            part_copy(k, j, peer).wait_send()
    for m in range(3):
        for c in range(n):
            for b in range(fs):
                k = tile_of(b, y, c)
                pl.when(has_up & (b <= z))(lambda k=k: hop(m, k, up_dev, up_sem).wait_send())
                pl.when(has_dn & (b >= z))(lambda k=k: hop(m, k, dn_dev, dn_sem).wait_send())
                pl.when(z != b)(lambda k=k: hop(m, k, y_dev, y_sem).wait_send())


def emit_kernel(fg, fu, fd, mixed_ref, pg_ref, pb_ref, go_ref, uo_ref, do_ref, res_ref, sem):
    tiles = fg.shape[0]
    copies = [
        pltpu.make_async_copy(src.at[k], out.at[:, k * LANES:(k + 1) * LANES], sem.at[m, k])
        for m, (src, out) in enumerate(((fg, go_ref), (fu, uo_ref), (fd, do_ref)))
        for k in range(tiles)
    ]
    for copy in copies:
        copy.start()
    mix = mixed_ref[...]
    center = jnp.mean(mix, axis=-1, keepdims=True)
    off = mix - center
    spread = jnp.mean(jnp.square(off), axis=-1, keepdims=True)
    res_ref[...] = (
        off * lax.rsqrt(spread + 1e-05) * pg_ref[...] + pb_ref[...]
    ).astype(jnp.bfloat16)
    for copy in copies:
        copy.wait()


def fused(fs, tp, n, tokens, gate_master, up_master, down_master, norm_gain, post_gain, post_bias):
    rc, cols = gate_master.shape
    tok_rows, d = tokens.shape
    tiles, rows = d // LANES, tp * tok_rows
    bf, f32 = jnp.bfloat16, jnp.float32
    held = pltpu.VMEM((tiles, cols, LANES), bf)
    vmem = pl.BlockSpec(memory_space=pltpu.VMEM)
    anywhere = pl.BlockSpec(memory_space=pl.ANY)
    dma = pltpu.SemaphoreType.DMA
    kept = pl.pallas_call(
        functools.partial(fused_kernel, fs, tp, n),
        out_shape=(held, held, held, pltpu.VMEM((tok_rows, d), f32)),
        in_specs=[vmem] + [anywhere] * 3 + [vmem],
        out_specs=(vmem,) * 4,
        scratch_shapes=[
            pltpu.VMEM((3, 2 * n, cols, LANES), f32),
            pltpu.VMEM((tp, tok_rows, d), bf),
            pltpu.VMEM((rows, cols), f32),
            pltpu.VMEM((rows, cols), f32),
            pltpu.VMEM((rows, cols), bf),
            pltpu.VMEM((tiles, rows, LANES), bf),
            pltpu.VMEM((tp, tiles, tok_rows, LANES), bf),
            dma((3 * tiles,)), dma((3 * tiles,)), dma((3 * tiles,)), dma((3 * tiles,)),
            dma((tp - 1,)), dma((tp,)),
            dma((tp - 1, tiles)), dma((tp, tiles)), dma((3, 2 * n)),
        ],
        compiler_params=pltpu.CompilerParams(
            collective_id=0, has_side_effects=True, vmem_limit_bytes=50 * 2**20
        ),
    )(
        tokens,
        *(
            pltpu.with_memory_space_constraint(x.T, pltpu.HBM)
            for x in (gate_master, up_master, down_master)
        ),
        norm_gain[None, :],
    )
    kept = [pltpu.with_memory_space_constraint(x, pltpu.VMEM) for x in kept]
    ready = jax.ShapeDtypeStruct((cols, d), bf)
    gate, up, down, result = pl.pallas_call(
        emit_kernel,
        out_shape=(ready, ready, ready, jax.ShapeDtypeStruct((tok_rows, d), bf)),
        in_specs=[vmem] * 6,
        out_specs=(anywhere, anywhere, anywhere, vmem),
        scratch_shapes=[dma((3, tiles))],
        compiler_params=pltpu.CompilerParams(vmem_limit_bytes=20 * 2**20),
    )(*kept, post_gain[None, :], post_bias[None, :])
    return gate.T, up.T, down.T, result


def solution(mesh):
    grp, fs, tp = mesh.shape["grp"], mesh.shape["fs"], mesh.shape["tp"]

    def local(tokens, gate_master, *rest):
        rc, cols = gate_master.shape
        n = rc // (2 * LANES)
        fits = grp == 2 and fs > 1 and rc % (2 * LANES) == 0 and 2 * n * fs <= 32
        fits = fits and cols % 16 == 0 and tokens.shape[0] % 16 == 0
        if fits:
            return fused(fs, tp, n, tokens, gate_master, *rest)
        return plain(tokens, gate_master, *rest)

    return jax.shard_map(
        local,
        mesh=mesh,
        in_specs=(
            P(("grp", "fs", "tp"), None),
            P("fs", "tp"),
            P("fs", "tp"),
            P("fs", "tp"),
            P(),
            P(),
            P(),
        ),
        out_specs=(P("grp", "tp"), P("grp", "tp"), P("grp", "tp"), P(("grp", "fs", "tp"), None)),
        check_vma=False,
    )
```

```python
import functools

import jax
import jax.numpy as jnp
from jax import lax
from jax.experimental import pallas as pl
from jax.experimental.pallas import tpu as pltpu
from jax.sharding import PartitionSpec as P

MESH = pl.DeviceIdType.MESH
LANES = 128
LAG = 3


def finish(wide, branch, post_gain, post_bias):
    mixed = jnp.sqrt(jnp.float32(2.0)) * wide + 0.5 * branch
    center = jnp.mean(mixed, axis=-1, keepdims=True)
    spread = jnp.mean(jnp.square(mixed - center), axis=-1, keepdims=True)
    return ((mixed - center) * lax.rsqrt(spread + 1e-05) * post_gain + post_bias).astype(
        jnp.bfloat16
    )


def plain(tokens, gate_master, up_master, down_master, norm_gain, post_gain, post_bias):
    row_count = gate_master.shape[0]
    first_row = lax.axis_index("fs") * row_count
    gain_rows = lax.dynamic_slice_in_dim(norm_gain, first_row, row_count, 0)
    gate_piece = (gain_rows[:, None] * gate_master).astype(jnp.bfloat16)
    up_piece = (gain_rows[:, None] * up_master).astype(jnp.bfloat16)
    down_piece = down_master.astype(jnp.bfloat16)
    gate_ready, up_ready, down_ready = (
        lax.all_gather(gate_piece, "fs", axis=0, tiled=True),
        lax.all_gather(up_piece, "fs", axis=0, tiled=True),
        lax.all_gather(down_piece, "fs", axis=0, tiled=True),
    )
    wide = tokens.astype(jnp.float32)
    normed = (wide * lax.rsqrt(jnp.mean(wide * wide, axis=-1, keepdims=True) + 1e-06)).astype(
        jnp.bfloat16
    )
    piece = lax.all_gather(normed, "tp", axis=0, tiled=True)
    gate = jnp.dot(piece, gate_ready, preferred_element_type=jnp.float32)
    upward = jnp.dot(piece, up_ready, preferred_element_type=jnp.float32)
    hidden = (jax.nn.silu(gate) * upward).astype(jnp.bfloat16)
    branch = lax.psum_scatter(
        lax.dot_general(
            hidden, down_ready, (((1,), (1,)), ((), ())), preferred_element_type=jnp.float32
        ).astype(jnp.bfloat16),
        "tp",
        scatter_dimension=0,
        tiled=True,
    ).astype(jnp.float32)
    result = finish(wide, branch, post_gain, post_bias)
    return (gate_ready, up_ready, down_ready, result)


def row_pieces(cols):
    return -(-cols // 32) * 16, cols * 3 // 8 // LANES * LANES


def gather_kernel(
    fs, tp, n, tok_ref, gm_ref, um_ref, dm_ref, gain_ref,
    fg, fu, fd, mixed,
    stage, own, gain, toks, acc_g, acc_u, hid, parts, got,
    up_sem, dn_sem, y_sem, r_sem, ts_sem, tr_sem, ps_sem, pr_sem, i_sem, l_sem,
):
    y, z, t = lax.axis_index("grp"), lax.axis_index("fs"), lax.axis_index("tp")
    cols, rc = gm_ref.shape
    tok_rows, d = tok_ref.shape
    tiles = d // LANES
    middle, split = row_pieces(cols)
    full = (fg, fu, fd)
    masters = (gm_ref, um_ref, dm_ref)
    up_dev = (y, jnp.minimum(z + 1, fs - 1), t)
    dn_dev = (y, jnp.maximum(z - 1, 0), t)
    y_dev = (1 - y, z, t)
    has_up, has_dn = z < fs - 1, z > 0
    at_end = jnp.logical_or(z == 0, z == fs - 1)
    far = fs - 1 - z
    peers = [lax.rem(t + j, tp) for j in range(1, tp)]
    senders = [lax.rem(t + tp - j, tp) for j in range(1, tp)]
    first = [(m, c) for m in (0, 1) for c in range(n)]
    second = [(2, c) for c in range(n)]

    barrier = pltpu.get_barrier_semaphore()

    def greet(dev):
        pl.semaphore_signal(barrier, inc=1, device_id=dev, device_id_type=MESH)

    pl.when(has_up)(lambda: greet(up_dev))
    pl.when(has_dn)(lambda: greet(dn_dev))
    greet(y_dev)
    for peer in peers:
        greet((y, z, peer))

    def pieces(m, c):
        if (m, c) == (2, n - 1):
            return [(0, 0, split), (1, split, cols - split)]
        return [(0, 0, middle), (1, middle, cols - middle)]

    def is_last(m, c, q):
        return (m, c, q[0]) == (2, n - 1, 1)

    def group(m, c, q):
        return m if (m, c) != (2, n - 1) else 3 + q[0]

    def fetch(m, h, c):
        k = h * n + c
        return pltpu.make_async_copy(
            masters[m].at[:, pl.ds(pl.multiple_of(k * LANES, LANES), LANES)],
            stage.at[m, k], i_sem.at[m, k],
        )

    gain_copy = pltpu.make_async_copy(gain_ref, gain, l_sem.at[0])
    tok_fetch = pltpu.make_async_copy(tok_ref, own, l_sem.at[1])
    gain_copy.start()
    for m, c in first:
        fetch(m, y, c).start()
    tok_fetch.start()
    for m, c in second:
        fetch(m, y, c).start()
    for m, c in first + second:
        fetch(m, 1 - y, c).start()

    def tile_of(b, h, c):
        return b * (2 * n) + h * n + c

    def hop(m, c, k, q, dev, sem, skip):
        rows = pl.ds(q[1], q[2])
        slot = (m * (fs - 1) - skip) * (2 * n) + k
        return pltpu.make_async_remote_copy(
            src_ref=full[m].at[k, rows], dst_ref=full[m].at[k, rows],
            send_sem=sem.at[group(m, c, q)], recv_sem=r_sem.at[slot, q[0]],
            device_id=dev, device_id_type=MESH,
        )

    def keep(m, h, c, q):
        if q[0] == 0:
            fetch(m, h, c).wait()
        k = tile_of(z, h, c)
        rows = pl.ds(q[1], q[2])
        v = stage[m, h * n + c, rows, :]
        if m < 2:
            v = v * gain[:, pl.ds(pl.multiple_of(k * LANES, LANES), LANES)]
        full[m][k, rows, :] = v.astype(jnp.bfloat16)

    def send_up(m, h, c, q):
        hop(m, c, tile_of(z, h, c), q, up_dev, up_sem, 0).start()

    def send_dn(m, h, c, q):
        hop(m, c, tile_of(z, h, c), q, dn_dev, dn_sem, 1).start()

    def send_own(m, c, q):
        pl.when(has_up)(lambda: send_up(m, y, c, q))
        pl.when(has_dn)(lambda: send_dn(m, y, c, q))

    def send_end(m, h, c, q):
        pl.when(z == 0)(lambda: send_up(m, h, c, q))
        pl.when(z == fs - 1)(lambda: send_dn(m, h, c, q))

    def part_slot(b, h, c):
        return b * 2 + h if c == 0 else 2 * fs + (c - 1) * 2 + h

    def part_copy(b, h, c, cnt, j, peer):
        k = tile_of(b, h, c)
        return pltpu.make_async_remote_copy(
            src_ref=parts.at[
                pl.ds(k, cnt), pl.ds(pl.multiple_of(peer * tok_rows, tok_rows), tok_rows)
            ],
            dst_ref=got.at[t, pl.ds(k, cnt)],
            send_sem=ps_sem.at[j], recv_sem=pr_sem.at[j, part_slot(b, h, c)],
            device_id=(y, z, peer), device_id_type=MESH,
        )

    def put_parts(ks, part):
        for i, k in enumerate(ks):
            parts[k] = part[:, i * LANES:(i + 1) * LANES].astype(jnp.bfloat16)

    def send_parts(b, h, c, cnt):
        for j, peer in enumerate(peers):
            part_copy(b, h, c, cnt, j, peer).start()

    def product(ks):
        rhs = jnp.concatenate([fd[k] for k in ks], axis=1)
        return jnp.dot(hid[...], rhs, preferred_element_type=jnp.float32)

    def down_half(b, h):
        ks = [tile_of(b, h, c) for c in range(n)]
        put_parts(ks, product(ks))
        send_parts(b, h, 0, n)

    def add_tiles(m, k, start):
        acc = (acc_g, acc_u)[m]
        at = pl.ds(pl.multiple_of(k * LANES, LANES), n * LANES)
        lhs = toks[:, :, at].reshape(tp * tok_rows, n * LANES)
        rhs = jnp.concatenate([full[m][k + i] for i in range(n)], axis=1)
        term = lax.dot_general(
            lhs, rhs, (((1,), (1,)), ((), ())), preferred_element_type=jnp.float32
        )
        acc[...] = term if start else acc[...] + term

    def finish_tiles(b, h, c, cnt):
        k = tile_of(b, h, c)
        for j, peer in enumerate(senders):
            dst = got.at[peer, pl.ds(k, cnt)]
            pltpu.make_async_remote_copy(
                src_ref=dst, dst_ref=dst, send_sem=ps_sem.at[j],
                recv_sem=pr_sem.at[j, part_slot(b, h, c)],
                device_id=(y, z, peer), device_id_type=MESH,
            ).wait_recv()
        mine = pl.ds(pl.multiple_of(t * tok_rows, tok_rows), tok_rows)
        for i in range(cnt):
            branch = parts[k + i, mine, :].astype(jnp.float32)
            for peer in senders:
                branch = branch + got[peer, k + i].astype(jnp.float32)
            at = pl.ds(pl.multiple_of((k + i) * LANES, LANES), LANES)
            wide = own[:, at].astype(jnp.float32)
            mixed[:, at] = jnp.sqrt(jnp.float32(2.0)) * wide + 0.5 * branch

    def ends(p):
        low, high = z - 1 - p, z + 1 + p
        return ((low, low >= 0, low == 0), (high, high <= fs - 1, high == fs - 1))

    sums, downs, fins = [], [], []

    def work(todo, count):
        for _ in range(min(count, len(todo))):
            ok, item = todo.pop(0)
            if ok is None:
                item()
            else:
                pl.when(ok)(item)

    def arrived(m, c, q, p):
        (low, has_low, low_end), (high, has_high, high_end) = ends(p)
        straight = p == 0 or is_last(m, c, q)

        def take(b, b_end, more, dev, sem, skip):
            k = tile_of(b, y, c)
            hop(m, c, k, q, dev, sem, skip).wait_recv()
            pl.when(more)(lambda: hop(m, c, k, q, dev, sem, skip).start())
            cross = lambda: hop(m, c, k, q, y_dev, y_sem, skip).start()
            if straight:
                pl.when(jnp.logical_not(b_end))(cross)
            else:
                cross()

        pl.when(has_low)(lambda: take(low, low_end, has_up, up_dev, up_sem, 0))
        pl.when(has_high)(lambda: take(high, high_end, has_dn, dn_dev, dn_sem, 1))

    def doubled(c, q, p):
        (low, has_low, low_end), (high, has_high, high_end) = ends(p)

        def take(b, more, dev, sem, skip):
            k = tile_of(b, 1 - y, c)
            hop(2, c, k, q, dev, sem, skip).wait_recv()
            pl.when(more)(lambda: hop(2, c, k, q, dev, sem, skip).start())

        pl.when(jnp.logical_and(has_low, low_end))(lambda: take(low, has_up, up_dev, up_sem, 0))
        pl.when(jnp.logical_and(has_high, high_end))(lambda: take(high, has_dn, dn_dev, dn_sem, 1))

    def crossed(m, c, p):
        for skip, (b, ok, b_end) in enumerate(ends(p)):
            k = tile_of(b, 1 - y, c)
            for q in pieces(m, c):
                here = jnp.logical_and(ok, jnp.logical_not(b_end)) if is_last(m, c, q) else ok
                pl.when(here)(
                    lambda k=k, q=q, skip=skip: hop(m, c, k, q, y_dev, y_sem, skip).wait_recv()
                )

    def later(m, c, p, h):
        if c < n - 1:
            return
        for b, ok, _ in ends(p):
            if m == 2:
                downs.append((ok, lambda b=b: down_half(b, h)))
                fins.append((ok, lambda b=b: finish_tiles(b, h, 0, n)))
            else:
                sums.append((ok, lambda b=b: add_tiles(m, tile_of(b, h, 0), False)))

    def tok_copy(j, peer, origin):
        return pltpu.make_async_remote_copy(
            src_ref=toks.at[origin], dst_ref=toks.at[origin],
            send_sem=ts_sem.at[j], recv_sem=tr_sem.at[j],
            device_id=(y, z, peer), device_id_type=MESH,
        )

    plan = [(m, c, q) for m, c in first for q in pieces(m, c)]
    gain_copy.wait()
    keep(plan[0][0], y, *plan[0][1:])
    expected = has_up.astype(jnp.int32) + has_dn.astype(jnp.int32) + tp
    pl.semaphore_wait(barrier, expected)
    for before, after in zip(plan, plan[1:]):
        keep(after[0], y, *after[1:])
        send_own(*before)
    tok_fetch.wait()
    wide = own[...].astype(jnp.float32)
    scale = lax.rsqrt(jnp.mean(wide * wide, axis=-1, keepdims=True) + 1e-06)
    send_own(*plan[-1])
    toks[t] = (wide * scale).astype(jnp.bfloat16)
    late = [(m, c, q) for m, c in second for q in pieces(m, c)]
    for m, c, q in late:
        keep(m, y, c, q)
    for j, peer in enumerate(peers):
        tok_copy(j, peer, t).start()
    for m, c, q in plan:
        keep(m, 1 - y, c, q)
    for m, c, q in plan:
        send_end(m, 1 - y, c, q)
    for m, c, q in late:
        send_end(m, y, c, q)
    for m, c, q in late:
        keep(m, 1 - y, c, q)
    for m, c, q in late:
        send_end(m, 1 - y, c, q)

    waiting = []

    def settle(count):
        while len(waiting) > count:
            m, c, p = waiting.pop(0)
            crossed(m, c, p)
            later(m, c, p, 1 - y)

    for p in range(fs - 1):
        for m, c in first:
            for q in pieces(m, c):
                arrived(m, c, q, p)
            later(m, c, p, y)
            waiting.append((m, c, p))
            settle(LAG)
            if p > 0:
                work(sums, 4)
        if p == 0:
            for j, peer in enumerate(senders):
                tok_copy(j, peer, peer).wait_recv()
            sums[:0] = [
                (None, lambda m=m, h=h: add_tiles(m, tile_of(z, h, 0), h == 0))
                for m in (0, 1) for h in (0, 1)
            ]

    @pl.when(jnp.logical_not(at_end))
    def _():
        for m, c, q in late:
            send_own(m, c, q)

    for p in range(fs - 2):
        for m, c in second:
            for q in pieces(m, c):
                arrived(m, c, q, p)
                if is_last(m, c, q):
                    doubled(c, q, p)
            if p == 0 and c == 0:
                settle(0)
                work(sums, len(sums))
                hid[...] = (jax.nn.silu(acc_g[...]) * acc_u[...]).astype(jnp.bfloat16)
                for h in (0, 1):
                    downs.append((None, lambda h=h: down_half(z, h)))
                    fins.append((None, lambda h=h: finish_tiles(z, h, 0, n)))
            later(m, c, p, y)
            waiting.append((m, c, p))
            settle(1)
            work(downs, 4)

    def far_tile(h, c):
        return tile_of(far, h, c)

    far_skip = (far > z).astype(jnp.int32)

    def far_take(c, q):
        k = far_tile(y, c)
        hop(2, c, k, q, y_dev, y_sem, far_skip).wait_recv()
        if not is_last(2, c, q):
            hop(2, c, k, q, y_dev, y_sem, far_skip).start()

    def far_cross(c, q):
        hop(2, c, far_tile(1 - y, c), q, y_dev, y_sem, far_skip).wait_recv()

    def far_down(c):
        ks = [far_tile(h, c) for h in (0, 1)]
        put_parts(ks, product(ks))
        for h in (0, 1):
            send_parts(far, h, c, 1)

    head = [(c, q) for _, c, q in late if c < n - 1]
    tail = [q for _, c, q in late if c == n - 1]

    @pl.when(at_end)
    def _():
        for c, q in head:
            far_take(c, q)

    settle(0)
    work(downs, len(downs))
    pl.when(at_end)(lambda: far_take(n - 1, tail[0]))
    work(fins, 4)

    @pl.when(at_end)
    def _():
        for c, q in head:
            far_cross(c, q)
        for c in range(n - 1):
            far_down(c)

    work(fins, len(fins))

    @pl.when(at_end)
    def _():
        far_take(n - 1, tail[1])
        far_cross(n - 1, tail[1])
        far_cross(n - 1, tail[0])
        far_down(n - 1)
        for c in range(n):
            for h in (0, 1):
                finish_tiles(far, h, c, 1)

    def sent(g, count, sem, dev):
        if count:
            rows = slice(0, cols) if g < 3 else slice(0, split) if g == 3 else slice(split, cols)
            ref = full[min(g, 2)].at[pl.ds(0, count), rows]
            pltpu.make_async_remote_copy(
                src_ref=ref, dst_ref=ref, send_sem=sem.at[g], recv_sem=r_sem.at[0, 0],
                device_id=dev, device_id_type=MESH,
            ).wait_send()

    def sends(j, g):
        base = (n, n, n - 1, 1, 1)[g]
        outer = (0, fs - 1)
        twice = lambda b: 2 * base if g == 4 and b in outer else base
        mine = 2 * base if j in outer else base
        up = mine + sum(twice(b) for b in range(j)) if j < fs - 1 else 0
        dn = mine + sum(twice(b) for b in range(j + 1, fs)) if j > 0 else 0
        cross = sum(
            base for b in range(fs)
            if b != j and not (b in outer and (abs(b - j) == 1 or g == 4))
        )
        return up, dn, cross

    for j in range(fs):
        @pl.when(z == j)
        def _(j=j):
            for g in range(5):
                up, dn, cross = sends(j, g)
                sent(g, up, up_sem, up_dev)
                sent(g, dn, dn_sem, dn_dev)
                sent(g, cross, y_sem, y_dev)

    for j, peer in enumerate(peers):
        tok_copy(j, peer, t).wait_send()
        ref = parts.at[:, pl.ds(0, tok_rows)]
        pltpu.make_async_remote_copy(
            src_ref=ref, dst_ref=ref, send_sem=ps_sem.at[j], recv_sem=pr_sem.at[j, 0],
            device_id=(y, z, peer), device_id_type=MESH,
        ).wait_send()


def emit_kernel(
    fg, fu, fd, mixed, pg_ref, pb_ref, go_ref, uo_ref, do_ref, res_ref, res, sem, res_sem
):
    tiles = fg.shape[0]
    copies = [
        pltpu.make_async_copy(src.at[k], out.at[:, k * LANES:(k + 1) * LANES], sem.at[m, k])
        for m, (src, out) in enumerate(((fg, go_ref), (fu, uo_ref), (fd, do_ref)))
        for k in range(tiles)
    ]
    for copy in copies:
        copy.start()
    mix = mixed[...]
    center = jnp.mean(mix, axis=-1, keepdims=True)
    off = mix - center
    spread = jnp.mean(jnp.square(off), axis=-1, keepdims=True)
    res[...] = (
        off * lax.rsqrt(spread + 1e-05) * pg_ref[...] + pb_ref[...]
    ).astype(jnp.bfloat16)
    put = pltpu.make_async_copy(res, res_ref, res_sem)
    put.start()
    for copy in copies:
        copy.wait()
    put.wait()


def fused(fs, tp, n, tokens, gate_master, up_master, down_master, norm_gain, post_gain, post_bias):
    rc, cols = gate_master.shape
    tok_rows, d = tokens.shape
    tiles, rows = d // LANES, tp * tok_rows
    bf, f32 = jnp.bfloat16, jnp.float32
    held = pltpu.VMEM((tiles, cols, LANES), bf)
    vmem = pl.BlockSpec(memory_space=pltpu.VMEM)
    anywhere = pl.BlockSpec(memory_space=pl.ANY)
    dma = pltpu.SemaphoreType.DMA
    sources = (tokens, gate_master.T, up_master.T, down_master.T, norm_gain[None, :])
    kept = pl.pallas_call(
        functools.partial(gather_kernel, fs, tp, n),
        out_shape=(held, held, held, pltpu.VMEM((tok_rows, d), f32)),
        in_specs=[anywhere] * 5,
        out_specs=(vmem,) * 4,
        scratch_shapes=[
            pltpu.VMEM((3, 2 * n, cols, LANES), f32),
            pltpu.VMEM((tok_rows, d), bf),
            pltpu.VMEM((1, d), f32),
            pltpu.VMEM((tp, tok_rows, d), bf),
            pltpu.VMEM((rows, cols), f32),
            pltpu.VMEM((rows, cols), f32),
            pltpu.VMEM((rows, cols), bf),
            pltpu.VMEM((tiles, rows, LANES), bf),
            pltpu.VMEM((tp, tiles, tok_rows, LANES), bf),
            dma((5,)), dma((5,)), dma((5,)), dma((3 * (fs - 1) * 2 * n, 2)),
            dma((tp - 1,)), dma((tp - 1,)), dma((tp - 1,)), dma((tp - 1, 2 * (fs + n - 1))),
            dma((3, 2 * n)), dma((2,)),
        ],
        compiler_params=pltpu.CompilerParams(
            collective_id=0, has_side_effects=True, vmem_limit_bytes=50 * 2**20
        ),
    )(*(pltpu.with_memory_space_constraint(x, pltpu.HBM) for x in sources))
    ready = jax.ShapeDtypeStruct((cols, d), bf)
    gate, up, down, result = pl.pallas_call(
        emit_kernel,
        out_shape=(ready, ready, ready, jax.ShapeDtypeStruct((tok_rows, d), bf)),
        in_specs=[vmem] * 6,
        out_specs=(anywhere,) * 4,
        scratch_shapes=[
            pltpu.VMEM((tok_rows, d), bf), dma((3, tiles)), pltpu.SemaphoreType.DMA,
        ],
        compiler_params=pltpu.CompilerParams(vmem_limit_bytes=20 * 2**20),
    )(
        *(pltpu.with_memory_space_constraint(x, pltpu.VMEM) for x in kept),
        post_gain[None, :], post_bias[None, :],
    )
    return gate.T, up.T, down.T, result


def solution(mesh):
    grp, fs, tp = mesh.shape["grp"], mesh.shape["fs"], mesh.shape["tp"]

    def local(tokens, gate_master, *rest):
        rc, cols = gate_master.shape
        n = rc // (2 * LANES)
        fits = grp == 2 and fs > 2 and rc % (2 * LANES) == 0 and 2 * n * fs <= 32
        fits = fits and cols % 16 == 0 and tokens.shape[0] % 16 == 0
        middle, split = row_pieces(cols)
        fits = fits and 0 < middle < cols and 0 < split < cols
        if fits:
            return fused(fs, tp, n, tokens, gate_master, *rest)
        return plain(tokens, gate_master, *rest)

    return jax.shard_map(
        local,
        mesh=mesh,
        in_specs=(
            P(("grp", "fs", "tp"), None),
            P("fs", "tp"),
            P("fs", "tp"),
            P("fs", "tp"),
            P(),
            P(),
            P(),
        ),
        out_specs=(P("grp", "tp"), P("grp", "tp"), P("grp", "tp"), P(("grp", "fs", "tp"), None)),
        check_vma=False,
    )
```

```python
import functools

import jax
import jax.numpy as jnp
from jax import lax
from jax.experimental import pallas as pl
from jax.experimental.pallas import tpu as pltpu
from jax.sharding import PartitionSpec as P

MESH = pl.DeviceIdType.MESH
LANES = 128
LAG = 3


def finish(wide, branch, post_gain, post_bias):
    mixed = jnp.sqrt(jnp.float32(2.0)) * wide + 0.5 * branch
    center = jnp.mean(mixed, axis=-1, keepdims=True)
    spread = jnp.mean(jnp.square(mixed - center), axis=-1, keepdims=True)
    return ((mixed - center) * lax.rsqrt(spread + 1e-05) * post_gain + post_bias).astype(
        jnp.bfloat16
    )


def plain(tokens, gate_master, up_master, down_master, norm_gain, post_gain, post_bias):
    row_count = gate_master.shape[0]
    first_row = lax.axis_index("fs") * row_count
    gain_rows = lax.dynamic_slice_in_dim(norm_gain, first_row, row_count, 0)
    gate_piece = (gain_rows[:, None] * gate_master).astype(jnp.bfloat16)
    up_piece = (gain_rows[:, None] * up_master).astype(jnp.bfloat16)
    down_piece = down_master.astype(jnp.bfloat16)
    gate_ready, up_ready, down_ready = (
        lax.all_gather(gate_piece, "fs", axis=0, tiled=True),
        lax.all_gather(up_piece, "fs", axis=0, tiled=True),
        lax.all_gather(down_piece, "fs", axis=0, tiled=True),
    )
    wide = tokens.astype(jnp.float32)
    normed = (wide * lax.rsqrt(jnp.mean(wide * wide, axis=-1, keepdims=True) + 1e-06)).astype(
        jnp.bfloat16
    )
    piece = lax.all_gather(normed, "tp", axis=0, tiled=True)
    gate = jnp.dot(piece, gate_ready, preferred_element_type=jnp.float32)
    upward = jnp.dot(piece, up_ready, preferred_element_type=jnp.float32)
    hidden = (jax.nn.silu(gate) * upward).astype(jnp.bfloat16)
    branch = lax.psum_scatter(
        lax.dot_general(
            hidden, down_ready, (((1,), (1,)), ((), ())), preferred_element_type=jnp.float32
        ).astype(jnp.bfloat16),
        "tp",
        scatter_dimension=0,
        tiled=True,
    ).astype(jnp.float32)
    result = finish(wide, branch, post_gain, post_bias)
    return (gate_ready, up_ready, down_ready, result)


def gather_kernel(
    fs, tp, n, tok_ref, gm_ref, um_ref, dm_ref, gain_ref,
    fg, fu, fd, mixed,
    stage, own, gain, toks, acc_g, acc_u, hid, parts, got,
    hid_far, parts_far, got_far, sum_far, branch_far,
    up_sem, dn_sem, y_sem, r_sem, x_sem, t_sem, ps_sem, pr_sem, i_sem, l_sem, h_sem, p_sem, b_sem,
):
    y, z, t = lax.axis_index("grp"), lax.axis_index("fs"), lax.axis_index("tp")
    cols, rc = gm_ref.shape
    tok_rows, d = tok_ref.shape
    tiles = d // LANES
    middle = -(-cols // 32) * 16
    pieces = ((0, 0, middle), (1, middle, cols - middle))
    full = (fg, fu, fd)
    masters = (gm_ref, um_ref, dm_ref)
    up_dev = (y, jnp.minimum(z + 1, fs - 1), t)
    dn_dev = (y, jnp.maximum(z - 1, 0), t)
    y_dev = (1 - y, z, t)
    has_up, has_dn = z < fs - 1, z > 0
    at_end = jnp.logical_or(z == 0, z == fs - 1)
    by_end = jnp.logical_or(z == 1, z == fs - 2)
    far = jnp.where(z < 2, fs - 1, 0)
    cross = 1 - y
    end_dev = (y, jnp.where(z == 1, 0, fs - 1), t)
    helper = (y, jnp.where(z == 0, 1, fs - 2), t)
    peers = [lax.rem(t + j, tp) for j in range(1, tp)]
    senders = [lax.rem(t + tp - j, tp) for j in range(1, tp)]
    first = [(m, c) for m in (0, 1) for c in range(n)]
    second = [(2, c) for c in range(n)]

    barrier = pltpu.get_barrier_semaphore()

    def greet(dev):
        pl.semaphore_signal(barrier, inc=1, device_id=dev, device_id_type=MESH)

    pl.when(has_up)(lambda: greet(up_dev))
    pl.when(has_dn)(lambda: greet(dn_dev))
    greet(y_dev)
    for peer in peers:
        greet((y, z, peer))

    def is_last(m, c, q):
        return (m, c, q[0]) == (2, n - 1, 1)

    def group(m, c, q):
        return m if (m, c) != (2, n - 1) else 3 + q[0]

    def fetch(m, h, c, slot):
        k = h * n + c
        return pltpu.make_async_copy(
            masters[m].at[:, pl.ds(pl.multiple_of(k * LANES, LANES), LANES)],
            stage.at[m, k], i_sem.at[slot],
        )

    def fetched(m, h, c):
        if h is not y:
            if (m, c) == first[0]:
                ref = stage.at[:, pl.ds(h * n, n)]
                pltpu.make_async_copy(ref, ref, i_sem.at[2 * n + 1]).wait()
        elif m == 2:
            if c == 0:
                ref = stage.at[2, pl.ds(h * n, n)]
                pltpu.make_async_copy(ref, ref, i_sem.at[2 * n]).wait()
        else:
            fetch(m, h, c, m * n + c).wait()

    gain_copy = pltpu.make_async_copy(gain_ref, gain, l_sem.at[0])
    tok_fetch = pltpu.make_async_copy(tok_ref, own, l_sem.at[1])
    gain_copy.start()
    fetch(first[0][0], y, first[0][1], 0).start()

    def tile_of(b, h, c):
        return b * (2 * n) + h * n + c

    def hop(m, c, k, q, dev, sem, skip, other=False):
        rows = pl.ds(q[1], q[2])
        b = k // (2 * n)
        if other:
            recv_sem = x_sem.at[b - skip, group(m, c, q)]
        else:
            recv_sem = r_sem.at[(m * (fs - 1) + b - skip) * n + c, q[0]]
        return pltpu.make_async_remote_copy(
            src_ref=full[m].at[k, rows], dst_ref=full[m].at[k, rows],
            send_sem=sem.at[group(m, c, q)], recv_sem=recv_sem,
            device_id=dev, device_id_type=MESH,
        )

    def crossed_all(m, b, g, skip):
        k = tile_of(b, cross, 0)
        if g < 3:
            ref = full[m].at[pl.ds(k, (n, n, n - 1)[g])]
        else:
            q = pieces[g - 3]
            ref = full[2].at[k + n - 1, pl.ds(q[1], q[2])]
        pltpu.make_async_remote_copy(
            src_ref=ref, dst_ref=ref, send_sem=y_sem.at[g], recv_sem=x_sem.at[b - skip, g],
            device_id=y_dev, device_id_type=MESH,
        ).wait_recv()

    def keep(m, h, c, q):
        if q[0] == 0:
            fetched(m, h, c)
        k = tile_of(z, h, c)
        rows = pl.ds(q[1], q[2])
        v = stage[m, h * n + c, rows, :]
        if m < 2:
            v = v * gain[:, pl.ds(pl.multiple_of(k * LANES, LANES), LANES)]
        full[m][k, rows, :] = v.astype(jnp.bfloat16)

    def send_up(m, h, c, q):
        hop(m, c, tile_of(z, h, c), q, up_dev, up_sem, 0, h is not y).start()

    def send_dn(m, h, c, q):
        hop(m, c, tile_of(z, h, c), q, dn_dev, dn_sem, 1, h is not y).start()

    def part_copy(b, h, j, peer):
        k = tile_of(b, h, 0)
        return pltpu.make_async_remote_copy(
            src_ref=parts.at[
                pl.ds(k, n), pl.ds(pl.multiple_of(peer * tok_rows, tok_rows), tok_rows)
            ],
            dst_ref=got.at[t, pl.ds(k, n)],
            send_sem=ps_sem.at[0], recv_sem=pr_sem.at[b],
            device_id=(y, z, peer), device_id_type=MESH,
        )

    def product(lhs, k, to, at):
        rhs = jnp.concatenate([fd[k + i] for i in range(n)], axis=1)
        part = jnp.dot(lhs[...], rhs, preferred_element_type=jnp.float32)
        for i in range(n):
            to[at + i] = part[:, i * LANES:(i + 1) * LANES].astype(jnp.bfloat16)

    def down_half(b, h):
        k = tile_of(b, h, 0)
        product(hid, k, parts, k)
        for j, peer in enumerate(peers):
            part_copy(b, h, j, peer).start()

    def add_tiles(m, k, start):
        acc = (acc_g, acc_u)[m]
        at = pl.ds(pl.multiple_of(k * LANES, LANES), n * LANES)
        lhs = toks[:, :, at].reshape(tp * tok_rows, n * LANES)
        rhs = jnp.concatenate([full[m][k + i] for i in range(n)], axis=1)
        term = lax.dot_general(
            lhs, rhs, (((1,), (1,)), ((), ())), preferred_element_type=jnp.float32
        )
        acc[...] = term if start else acc[...] + term

    mine = pl.ds(pl.multiple_of(t * tok_rows, tok_rows), tok_rows)

    def mix(k, branch):
        at = pl.ds(pl.multiple_of(k * LANES, LANES), LANES)
        wide = own[:, at].astype(jnp.float32)
        mixed[:, at] = jnp.sqrt(jnp.float32(2.0)) * wide + 0.5 * branch

    def finish_origin(b):
        k = tile_of(b, 0, 0)
        ref = got.at[pl.ds(0, tp - 1), pl.ds(k, 2 * n)]
        pltpu.make_async_remote_copy(
            src_ref=ref, dst_ref=ref, send_sem=ps_sem.at[0], recv_sem=pr_sem.at[b],
            device_id=y_dev, device_id_type=MESH,
        ).wait_recv()
        for i in range(2 * n):
            branch = parts[k + i, mine, :].astype(jnp.float32)
            for peer in senders:
                branch = branch + got[peer, k + i].astype(jnp.float32)
            mix(k + i, branch)

    hid_copy = pltpu.make_async_remote_copy(
        src_ref=hid, dst_ref=hid_far, send_sem=h_sem.at[0], recv_sem=h_sem.at[1],
        device_id=helper, device_id_type=MESH,
    )
    sum_copy = pltpu.make_async_remote_copy(
        src_ref=sum_far, dst_ref=branch_far, send_sem=b_sem.at[0], recv_sem=b_sem.at[1],
        device_id=end_dev, device_id_type=MESH,
    )

    def far_copy(j, peer):
        return pltpu.make_async_remote_copy(
            src_ref=parts_far.at[
                :, pl.ds(pl.multiple_of(peer * tok_rows, tok_rows), tok_rows)
            ],
            dst_ref=got_far.at[j], send_sem=p_sem.at[0], recv_sem=p_sem.at[1],
            device_id=(y, z, peer), device_id_type=MESH,
        )

    def help_down():
        hid_copy.wait_recv()
        for h in (0, 1):
            product(hid_far, tile_of(far, h, 0), parts_far, h * n)
        for j, peer in enumerate(peers):
            far_copy(j, peer).start()

    def help_sum():
        pltpu.make_async_remote_copy(
            src_ref=got_far, dst_ref=got_far, send_sem=p_sem.at[0], recv_sem=p_sem.at[1],
            device_id=y_dev, device_id_type=MESH,
        ).wait_recv()
        total = parts_far[:, mine, :].astype(jnp.float32)
        for j in range(tp - 1):
            total = total + got_far[j].astype(jnp.float32)
        sum_far[...] = total.astype(jnp.bfloat16)
        sum_copy.start()

    def ends(p):
        low, high = z - 1 - p, z + 1 + p
        return ((low, low >= 0, low == 0), (high, high <= fs - 1, high == fs - 1))

    sums, downs, fins = [], [], []

    def work(todo, count):
        for _ in range(min(count, len(todo))):
            ok, item = todo.pop(0)
            if ok is None:
                item()
            else:
                pl.when(ok)(item)

    def take(m, c, q, b, b_end, more, dev, sem, skip, straight):
        k = tile_of(b, y, c)
        hop(m, c, k, q, dev, sem, skip).wait_recv()
        pl.when(more)(lambda: hop(m, c, k, q, dev, sem, skip).start())
        pass_on = lambda: hop(m, c, k, q, y_dev, y_sem, skip, True).start()
        if straight:
            pl.when(jnp.logical_not(b_end))(pass_on)
        else:
            pass_on()

    def arrived_dn(m, c, q, p):
        _, (high, ok, b_end) = ends(p)
        straight = p == 0 or is_last(m, c, q)
        pl.when(ok)(lambda: take(m, c, q, high, b_end, has_dn, dn_dev, dn_sem, 1, straight))

    def arrived_up(m, c, q, p):
        (low, ok, b_end), _ = ends(p)
        straight = p == 0 or is_last(m, c, q)
        pl.when(ok)(lambda: take(m, c, q, low, b_end, has_up, up_dev, up_sem, 0, straight))

    def arrived(m, c, q, p):
        arrived_dn(m, c, q, p)
        arrived_up(m, c, q, p)

    def doubled(c, q, p):
        def take_other(b, more, dev, sem, skip):
            crossed_all(2, b, 4, skip)
            k = tile_of(b, cross, c)
            pl.when(more)(lambda: hop(2, c, k, q, dev, sem, skip, True).start())

        (low, has_low, low_end), (high, has_high, high_end) = ends(p)
        pl.when(jnp.logical_and(has_high, high_end))(
            lambda: take_other(high, has_dn, dn_dev, dn_sem, 1)
        )
        pl.when(jnp.logical_and(has_low, low_end))(
            lambda: take_other(low, has_up, up_dev, up_sem, 0)
        )

    def crossed(m, c, p):
        groups = {n - 1: (m,) if m < 2 else (3, 4), n - 2: () if m < 2 else (2,)}.get(c, ())
        for skip, (b, ok, b_end) in enumerate(ends(p)):
            for g in groups:
                here = jnp.logical_and(ok, jnp.logical_not(b_end)) if g == 4 else ok
                pl.when(here)(lambda b=b, g=g, skip=skip: crossed_all(m, b, g, skip))

    def later(m, c, p, h):
        if c < n - 1:
            return
        for b, ok, _ in ends(p):
            if m == 2:
                downs.append((ok, lambda b=b: down_half(b, h)))
                if h is not y:
                    fins.append((ok, lambda b=b: finish_origin(b)))
            else:
                sums.append((ok, lambda b=b: add_tiles(m, tile_of(b, h, 0), False)))

    def tok_copy(peer, origin):
        return pltpu.make_async_remote_copy(
            src_ref=toks.at[origin], dst_ref=toks.at[origin],
            send_sem=t_sem.at[0], recv_sem=t_sem.at[1],
            device_id=(y, z, peer), device_id_type=MESH,
        )

    plan = [(m, c, q) for m, c in first for q in pieces]
    gain_copy.wait()
    keep(plan[0][0], y, *plan[0][1:])
    for m, c in first[1:]:
        fetch(m, y, c, m * n + c).start()
    tok_fetch.start()
    for m, c in second:
        fetch(m, y, c, 2 * n).start()
    for m, c in first + second:
        fetch(m, cross, c, 2 * n + 1).start()
    pl.semaphore_wait(barrier, has_up.astype(jnp.int32) + has_dn.astype(jnp.int32) + tp)
    tok_all = pltpu.make_async_remote_copy(
        src_ref=toks.at[pl.ds(0, tp - 1)], dst_ref=toks.at[pl.ds(0, tp - 1)],
        send_sem=t_sem.at[0], recv_sem=t_sem.at[1], device_id=y_dev, device_id_type=MESH,
    )
    late = [(m, c, q) for m, c in second for q in pieces]

    def send_own(m, c, q):
        pl.when(has_dn)(lambda: send_dn(m, y, c, q))
        pl.when(has_up)(lambda: send_up(m, y, c, q))

    for before, after in zip(plan, plan[1:]):
        keep(after[0], y, *after[1:])
        send_own(*before)
    tok_fetch.wait()
    wide = own[...].astype(jnp.float32)
    scale = lax.rsqrt(jnp.mean(wide * wide, axis=-1, keepdims=True) + 1e-06)
    send_own(*plan[-1])
    toks[t] = (wide * scale).astype(jnp.bfloat16)
    for m, c, q in late:
        keep(m, y, c, q)
    for peer in peers:
        tok_copy(peer, t).start()
    for m, c, q in plan + late:
        keep(m, cross, c, q)
    order = [(m, cross, c, q) for m, c, q in plan]
    order += [(m, y, c, q) for m, c, q in late]
    order += [(m, cross, c, q) for m, c, q in late]

    @pl.when(z == fs - 1)
    def _():
        for item in order:
            send_dn(*item)

    @pl.when(z == 0)
    def _():
        for item in order:
            send_up(*item)

    waiting = []

    def settle(count):
        while len(waiting) > count:
            m, c, p = waiting.pop(0)
            crossed(m, c, p)
            later(m, c, p, cross)

    for p in range(fs - 1):
        for m, c in first:
            for q in pieces:
                arrived(m, c, q, p)
            later(m, c, p, y)
            waiting.append((m, c, p))
            settle(LAG)
            if p > 0:
                work(sums, 4)
        if p == 0:
            tok_all.wait_recv()
            sums[:0] = [
                (None, lambda m=m, h=h: add_tiles(m, tile_of(z, h, 0), h == 0))
                for m in (0, 1) for h in (0, 1)
            ]

    @pl.when(jnp.logical_not(at_end))
    def _():
        for m, c, q in late:
            send_own(m, c, q)

    for p in range(fs - 2):
        for m, c in second:
            for q in pieces:
                arrived(m, c, q, p)
                if is_last(m, c, q):
                    doubled(c, q, p)
            if p == 0 and c == 0:
                settle(0)
                work(sums, len(sums))
                hid[...] = (jax.nn.silu(acc_g[...]) * acc_u[...]).astype(jnp.bfloat16)
                pl.when(at_end)(hid_copy.start)
                for h in (0, 1):
                    downs.append((None, lambda h=h: down_half(z, h)))
                fins.append((None, lambda: finish_origin(z)))
            later(m, c, p, y)
            waiting.append((m, c, p))
            settle(1)
            work(downs, 4)

    def far_tile(h, c):
        return tile_of(far, h, c)

    far_skip = (far > z).astype(jnp.int32)

    def far_take(c, q):
        k = far_tile(y, c)
        hop(2, c, k, q, y_dev, y_sem, far_skip).wait_recv()
        if not is_last(2, c, q):
            hop(2, c, k, q, y_dev, y_sem, far_skip, True).start()

    @pl.when(at_end)
    def _():
        for _, c, q in late[:-1]:
            far_take(c, q)

    settle(0)
    work(downs, len(downs))
    pl.when(by_end)(help_down)
    work(fins, len(fins))
    pl.when(by_end)(help_sum)

    @pl.when(at_end)
    def _():
        far_take(*late[-1][1:])
        for g in (2, 3, 4) if n > 1 else (3, 4):
            crossed_all(2, far, g, far_skip)
        sum_copy.wait_recv()
        for i in range(2 * n):
            mix(far * (2 * n) + i, branch_far[i].astype(jnp.float32))

    def sent(g, count, sem, dev):
        if count:
            rows = (slice(0, cols),) * 3 + (slice(0, middle), slice(middle, cols))
            rows = rows[g]
            ref = full[min(g, 2)].at[pl.ds(0, count), rows]
            pltpu.make_async_remote_copy(
                src_ref=ref, dst_ref=ref, send_sem=sem.at[g], recv_sem=b_sem.at[1],
                device_id=dev, device_id_type=MESH,
            ).wait_send()

    def sends(j, g):
        base = (n, n, n - 1, 1, 1)[g]
        outer = (0, fs - 1)
        twice = lambda b: 2 * base if g == 4 and b in outer else base
        mine = 2 * base if j in outer else base
        up = mine + sum(twice(b) for b in range(j)) if j < fs - 1 else 0
        dn = mine + sum(twice(b) for b in range(j + 1, fs)) if j > 0 else 0
        cross = sum(
            base for b in range(fs)
            if b != j and not (b in outer and (abs(b - j) == 1 or g == 4))
        )
        return up, dn, cross

    for j in range(fs):
        @pl.when(z == j)
        def _(j=j):
            for g in range(5):
                up, dn, cross = sends(j, g)
                sent(g, up, up_sem, up_dev)
                sent(g, dn, dn_sem, dn_dev)
                sent(g, cross, y_sem, y_dev)

    def shared(ref, sem):
        return pltpu.make_async_remote_copy(
            src_ref=ref, dst_ref=ref, send_sem=sem.at[0], recv_sem=b_sem.at[1],
            device_id=y_dev, device_id_type=MESH,
        )

    tok_all.wait_send()
    others = pl.ds(0, (tp - 1) * tok_rows)
    pl.when(at_end)(shared(parts.at[pl.ds(0, tiles - 2 * n), others], ps_sem).wait_send)
    pl.when(jnp.logical_not(at_end))(shared(parts.at[:, others], ps_sem).wait_send)
    pl.when(by_end)(shared(parts_far.at[:, others], p_sem).wait_send)
    pl.when(at_end)(hid_copy.wait_send)
    pl.when(by_end)(sum_copy.wait_send)


def emit_kernel(
    fg, fu, fd, mixed, pg_ref, pb_ref, go_ref, uo_ref, do_ref, res_ref, res, sem, res_sem
):
    tiles = fg.shape[0]
    copies = [
        pltpu.make_async_copy(src.at[k], out.at[:, k * LANES:(k + 1) * LANES], sem.at[m, k])
        for m, (src, out) in enumerate(((fg, go_ref), (fu, uo_ref), (fd, do_ref)))
        for k in range(tiles)
    ]
    for copy in copies:
        copy.start()
    mix = mixed[...]
    center = jnp.mean(mix, axis=-1, keepdims=True)
    off = mix - center
    spread = jnp.mean(jnp.square(off), axis=-1, keepdims=True)
    res[...] = (
        off * lax.rsqrt(spread + 1e-05) * pg_ref[...] + pb_ref[...]
    ).astype(jnp.bfloat16)
    put = pltpu.make_async_copy(res, res_ref, res_sem)
    put.start()
    for copy in copies:
        copy.wait()
    put.wait()


def fused(fs, tp, n, tokens, gate_master, up_master, down_master, norm_gain, post_gain, post_bias):
    rc, cols = gate_master.shape
    tok_rows, d = tokens.shape
    tiles, rows = d // LANES, tp * tok_rows
    bf, f32 = jnp.bfloat16, jnp.float32
    held = pltpu.VMEM((tiles, cols, LANES), bf)
    vmem = pl.BlockSpec(memory_space=pltpu.VMEM)
    anywhere = pl.BlockSpec(memory_space=pl.ANY)
    dma = pltpu.SemaphoreType.DMA
    sources = (tokens, gate_master.T, up_master.T, down_master.T, norm_gain[None, :])
    kept = pl.pallas_call(
        functools.partial(gather_kernel, fs, tp, n),
        out_shape=(held, held, held, pltpu.VMEM((tok_rows, d), f32)),
        in_specs=[anywhere] * 5,
        out_specs=(vmem,) * 4,
        scratch_shapes=[
            pltpu.VMEM((3, 2 * n, cols, LANES), f32),
            pltpu.VMEM((tok_rows, d), bf),
            pltpu.VMEM((1, d), f32),
            pltpu.VMEM((tp, tok_rows, d), bf),
            pltpu.VMEM((rows, cols), f32),
            pltpu.VMEM((rows, cols), f32),
            pltpu.VMEM((rows, cols), bf),
            pltpu.VMEM((tiles, rows, LANES), bf),
            pltpu.VMEM((tp, tiles, tok_rows, LANES), bf),
            pltpu.VMEM((rows, cols), bf),
            pltpu.VMEM((2 * n, rows, LANES), bf),
            pltpu.VMEM((tp - 1, 2 * n, tok_rows, LANES), bf),
            pltpu.VMEM((2 * n, tok_rows, LANES), bf),
            pltpu.VMEM((2 * n, tok_rows, LANES), bf),
            dma((5,)), dma((5,)), dma((5,)), dma((3 * (fs - 1) * n, 2)), dma((fs - 1, 5)),
            dma((2,)), dma((1,)), dma((fs,)), dma((2 * n + 2,)), dma((2,)),
            dma((2,)), dma((2,)), dma((2,)),
        ],
        compiler_params=pltpu.CompilerParams(
            collective_id=0, has_side_effects=True, vmem_limit_bytes=50 * 2**20
        ),
    )(*(pltpu.with_memory_space_constraint(x, pltpu.HBM) for x in sources))
    ready = jax.ShapeDtypeStruct((cols, d), bf)
    gate, up, down, result = pl.pallas_call(
        emit_kernel,
        out_shape=(ready, ready, ready, jax.ShapeDtypeStruct((tok_rows, d), bf)),
        in_specs=[vmem] * 6,
        out_specs=(anywhere,) * 4,
        scratch_shapes=[
            pltpu.VMEM((tok_rows, d), bf), dma((3, tiles)), pltpu.SemaphoreType.DMA,
        ],
        compiler_params=pltpu.CompilerParams(vmem_limit_bytes=20 * 2**20),
    )(
        *(pltpu.with_memory_space_constraint(x, pltpu.VMEM) for x in kept),
        post_gain[None, :], post_bias[None, :],
    )
    return gate.T, up.T, down.T, result


def solution(mesh):
    grp, fs, tp = mesh.shape["grp"], mesh.shape["fs"], mesh.shape["tp"]

    def local(tokens, gate_master, *rest):
        rc, cols = gate_master.shape
        n = rc // (2 * LANES)
        fits = grp == 2 and fs > 3 and rc % (2 * LANES) == 0 and 2 * n * fs <= 32
        fits = fits and cols % 16 == 0 and tokens.shape[0] % 16 == 0
        fits = fits and cols >= 2 * LANES
        if fits:
            return fused(fs, tp, n, tokens, gate_master, *rest)
        return plain(tokens, gate_master, *rest)

    return jax.shard_map(
        local,
        mesh=mesh,
        in_specs=(
            P(("grp", "fs", "tp"), None),
            P("fs", "tp"),
            P("fs", "tp"),
            P("fs", "tp"),
            P(),
            P(),
            P(),
        ),
        out_specs=(P("grp", "tp"), P("grp", "tp"), P("grp", "tp"), P(("grp", "fs", "tp"), None)),
        check_vma=False,
    )
```

```python
import functools

import jax
import jax.numpy as jnp
from jax import lax
from jax.experimental import pallas as pl
from jax.experimental.pallas import tpu as pltpu
from jax.sharding import PartitionSpec as P

MESH = pl.DeviceIdType.MESH
LANES = 128
LAG = 3


def finish(wide, branch, post_gain, post_bias):
    mixed = jnp.sqrt(jnp.float32(2.0)) * wide + 0.5 * branch
    center = jnp.mean(mixed, axis=-1, keepdims=True)
    spread = jnp.mean(jnp.square(mixed - center), axis=-1, keepdims=True)
    return ((mixed - center) * lax.rsqrt(spread + 1e-05) * post_gain + post_bias).astype(
        jnp.bfloat16
    )


def plain(tokens, gate_master, up_master, down_master, norm_gain, post_gain, post_bias):
    row_count = gate_master.shape[0]
    first_row = lax.axis_index("fs") * row_count
    gain_rows = lax.dynamic_slice_in_dim(norm_gain, first_row, row_count, 0)
    gate_piece = (gain_rows[:, None] * gate_master).astype(jnp.bfloat16)
    up_piece = (gain_rows[:, None] * up_master).astype(jnp.bfloat16)
    down_piece = down_master.astype(jnp.bfloat16)
    gate_ready, up_ready, down_ready = (
        lax.all_gather(gate_piece, "fs", axis=0, tiled=True),
        lax.all_gather(up_piece, "fs", axis=0, tiled=True),
        lax.all_gather(down_piece, "fs", axis=0, tiled=True),
    )
    wide = tokens.astype(jnp.float32)
    normed = (wide * lax.rsqrt(jnp.mean(wide * wide, axis=-1, keepdims=True) + 1e-06)).astype(
        jnp.bfloat16
    )
    piece = lax.all_gather(normed, "tp", axis=0, tiled=True)
    gate = jnp.dot(piece, gate_ready, preferred_element_type=jnp.float32)
    upward = jnp.dot(piece, up_ready, preferred_element_type=jnp.float32)
    hidden = (jax.nn.silu(gate) * upward).astype(jnp.bfloat16)
    branch = lax.psum_scatter(
        lax.dot_general(
            hidden, down_ready, (((1,), (1,)), ((), ())), preferred_element_type=jnp.float32
        ).astype(jnp.bfloat16),
        "tp",
        scatter_dimension=0,
        tiled=True,
    ).astype(jnp.float32)
    result = finish(wide, branch, post_gain, post_bias)
    return (gate_ready, up_ready, down_ready, result)


def gather_kernel(
    fs, tp, n, tok_ref, gm_ref, um_ref, dm_ref, gain_ref,
    fg, fu, fd, mixed,
    stage, own, gain, toks, acc_g, acc_u, hid, parts, got,
    hid_far, parts_far, got_far, sum_far, branch_far,
    up_sem, dn_sem, y_sem, r_sem, x_sem, t_sem, ps_sem, pr_sem, i_sem, l_sem, h_sem, p_sem, b_sem,
):
    y, z, t = lax.axis_index("grp"), lax.axis_index("fs"), lax.axis_index("tp")
    cols, rc = gm_ref.shape
    tok_rows, d = tok_ref.shape
    tiles = d // LANES
    middle = -(-cols // 32) * 16
    pieces = ((0, 0, middle), (1, middle, cols - middle))
    full = (fg, fu, fd)
    masters = (gm_ref, um_ref, dm_ref)
    up_dev = (y, jnp.minimum(z + 1, fs - 1), t)
    dn_dev = (y, jnp.maximum(z - 1, 0), t)
    y_dev = (1 - y, z, t)
    has_up, has_dn = z < fs - 1, z > 0
    at_end = jnp.logical_or(z == 0, z == fs - 1)
    by_end = jnp.logical_or(z == 1, z == fs - 2)
    far = jnp.where(z < 2, fs - 1, 0)
    cross = 1 - y
    end_dev = (y, jnp.where(z == 1, 0, fs - 1), t)
    helper = (y, jnp.where(z == 0, 1, fs - 2), t)
    peers = [lax.rem(t + j, tp) for j in range(1, tp)]
    senders = [lax.rem(t + tp - j, tp) for j in range(1, tp)]
    first = [(m, c) for m in (0, 1) for c in range(n)]
    second = [(2, c) for c in range(n)]

    barrier = pltpu.get_barrier_semaphore()

    def greet(dev):
        pl.semaphore_signal(barrier, inc=1, device_id=dev, device_id_type=MESH)

    pl.when(has_up)(lambda: greet(up_dev))
    pl.when(has_dn)(lambda: greet(dn_dev))
    greet(y_dev)
    for peer in peers:
        greet((y, z, peer))

    def is_last(m, c, q):
        return (m, c, q[0]) == (2, n - 1, 1)

    def group(m, c, q):
        return m if (m, c) != (2, n - 1) else 3 + q[0]

    def fetch(m, h, c, slot):
        k = h * n + c
        return pltpu.make_async_copy(
            masters[m].at[:, pl.ds(pl.multiple_of(k * LANES, LANES), LANES)],
            stage.at[m, k], i_sem.at[slot],
        )

    def fetched(m, h, c):
        if h is not y:
            if (m, c) == first[0]:
                ref = stage.at[:, pl.ds(h * n, n)]
                pltpu.make_async_copy(ref, ref, i_sem.at[2 * n + 1]).wait()
        elif m == 2:
            if c == 0:
                ref = stage.at[2, pl.ds(h * n, n)]
                pltpu.make_async_copy(ref, ref, i_sem.at[2 * n]).wait()
        else:
            fetch(m, h, c, m * n + c).wait()

    gain_copy = pltpu.make_async_copy(gain_ref, gain, l_sem.at[0])
    tok_fetch = pltpu.make_async_copy(tok_ref, own, l_sem.at[1])
    gain_copy.start()
    fetch(first[0][0], y, first[0][1], 0).start()

    def tile_of(b, h, c):
        return b * (2 * n) + h * n + c

    def hop(m, c, k, q, dev, sem, skip, other=False):
        rows = pl.ds(q[1], q[2])
        b = k // (2 * n)
        if other:
            recv_sem = x_sem.at[b - skip, group(m, c, q)]
        else:
            recv_sem = r_sem.at[(m * (fs - 1) + b - skip) * n + c, q[0]]
        return pltpu.make_async_remote_copy(
            src_ref=full[m].at[k, rows], dst_ref=full[m].at[k, rows],
            send_sem=sem.at[group(m, c, q)], recv_sem=recv_sem,
            device_id=dev, device_id_type=MESH,
        )

    def crossed_all(m, b, g, skip):
        k = tile_of(b, cross, 0)
        if g < 3:
            ref = full[m].at[pl.ds(k, (n, n, n - 1)[g])]
        else:
            q = pieces[g - 3]
            ref = full[2].at[k + n - 1, pl.ds(q[1], q[2])]
        pltpu.make_async_remote_copy(
            src_ref=ref, dst_ref=ref, send_sem=y_sem.at[g], recv_sem=x_sem.at[b - skip, g],
            device_id=y_dev, device_id_type=MESH,
        ).wait_recv()

    def keep(m, h, c, q):
        if q[0] == 0:
            fetched(m, h, c)
        k = tile_of(z, h, c)
        rows = pl.ds(q[1], q[2])
        v = stage[m, h * n + c, rows, :]
        if m < 2:
            v = v * gain[:, pl.ds(pl.multiple_of(k * LANES, LANES), LANES)]
        full[m][k, rows, :] = v.astype(jnp.bfloat16)

    def send_up(m, h, c, q):
        hop(m, c, tile_of(z, h, c), q, up_dev, up_sem, 0, h is not y).start()

    def send_dn(m, h, c, q):
        hop(m, c, tile_of(z, h, c), q, dn_dev, dn_sem, 1, h is not y).start()

    def part_copy(b, h, j, peer):
        k = tile_of(b, h, 0)
        return pltpu.make_async_remote_copy(
            src_ref=parts.at[
                pl.ds(k, n), pl.ds(pl.multiple_of(peer * tok_rows, tok_rows), tok_rows)
            ],
            dst_ref=got.at[t, pl.ds(k, n)],
            send_sem=ps_sem.at[0], recv_sem=pr_sem.at[b],
            device_id=(y, z, peer), device_id_type=MESH,
        )

    def product(lhs, k, to, at):
        rhs = jnp.concatenate([fd[k + i] for i in range(n)], axis=1)
        part = jnp.dot(lhs[...], rhs, preferred_element_type=jnp.float32)
        for i in range(n):
            to[at + i] = part[:, i * LANES:(i + 1) * LANES].astype(jnp.bfloat16)

    def down_half(b, h):
        k = tile_of(b, h, 0)
        product(hid, k, parts, k)
        for j, peer in enumerate(peers):
            part_copy(b, h, j, peer).start()

    def add_tiles(m, k, start):
        acc = (acc_g, acc_u)[m]
        at = pl.ds(pl.multiple_of(k * LANES, LANES), n * LANES)
        lhs = toks[:, :, at].reshape(tp * tok_rows, n * LANES)
        rhs = jnp.concatenate([full[m][k + i] for i in range(n)], axis=1)
        term = lax.dot_general(
            lhs, rhs, (((1,), (1,)), ((), ())), preferred_element_type=jnp.float32
        )
        acc[...] = term if start else acc[...] + term

    mine = pl.ds(pl.multiple_of(t * tok_rows, tok_rows), tok_rows)

    def mix(k, branch):
        at = pl.ds(pl.multiple_of(k * LANES, LANES), LANES)
        wide = own[:, at].astype(jnp.float32)
        mixed[:, at] = jnp.sqrt(jnp.float32(2.0)) * wide + 0.5 * branch

    def finish_origin(b):
        k = tile_of(b, 0, 0)
        ref = got.at[pl.ds(0, tp - 1), pl.ds(k, 2 * n)]
        pltpu.make_async_remote_copy(
            src_ref=ref, dst_ref=ref, send_sem=ps_sem.at[0], recv_sem=pr_sem.at[b],
            device_id=y_dev, device_id_type=MESH,
        ).wait_recv()
        for i in range(2 * n):
            branch = parts[k + i, mine, :].astype(jnp.float32)
            for peer in senders:
                branch = branch + got[peer, k + i].astype(jnp.float32)
            mix(k + i, branch)

    hid_copy = pltpu.make_async_remote_copy(
        src_ref=hid, dst_ref=hid_far, send_sem=h_sem.at[0], recv_sem=h_sem.at[1],
        device_id=helper, device_id_type=MESH,
    )
    sum_copy = pltpu.make_async_remote_copy(
        src_ref=sum_far, dst_ref=branch_far, send_sem=b_sem.at[0], recv_sem=b_sem.at[1],
        device_id=end_dev, device_id_type=MESH,
    )

    def far_copy(j, peer):
        return pltpu.make_async_remote_copy(
            src_ref=parts_far.at[
                :, pl.ds(pl.multiple_of(peer * tok_rows, tok_rows), tok_rows)
            ],
            dst_ref=got_far.at[j], send_sem=p_sem.at[0], recv_sem=p_sem.at[1],
            device_id=(y, z, peer), device_id_type=MESH,
        )

    def help_down():
        hid_copy.wait_recv()
        for h in (0, 1):
            product(hid_far, tile_of(far, h, 0), parts_far, h * n)
        for j, peer in enumerate(peers):
            far_copy(j, peer).start()

    def help_sum():
        pltpu.make_async_remote_copy(
            src_ref=got_far, dst_ref=got_far, send_sem=p_sem.at[0], recv_sem=p_sem.at[1],
            device_id=y_dev, device_id_type=MESH,
        ).wait_recv()
        total = parts_far[:, mine, :].astype(jnp.float32)
        for j in range(tp - 1):
            total = total + got_far[j].astype(jnp.float32)
        sum_far[...] = total.astype(jnp.bfloat16)
        sum_copy.start()

    def ends(p):
        low, high = z - 1 - p, z + 1 + p
        return ((low, low >= 0, low == 0), (high, high <= fs - 1, high == fs - 1))

    sums, downs, fins = [], [], []

    def work(todo, count):
        for _ in range(min(count, len(todo))):
            ok, item = todo.pop(0)
            if ok is None:
                item()
            else:
                pl.when(ok)(item)

    def take(m, c, q, b, b_end, more, dev, sem, skip, straight):
        k = tile_of(b, y, c)
        hop(m, c, k, q, dev, sem, skip).wait_recv()
        pl.when(more)(lambda: hop(m, c, k, q, dev, sem, skip).start())
        pass_on = lambda: hop(m, c, k, q, y_dev, y_sem, skip, True).start()
        if straight:
            pl.when(jnp.logical_not(b_end))(pass_on)
        else:
            pass_on()

    def arrived_dn(m, c, q, p):
        _, (high, ok, b_end) = ends(p)
        straight = p == 0 or is_last(m, c, q)
        pl.when(ok)(lambda: take(m, c, q, high, b_end, has_dn, dn_dev, dn_sem, 1, straight))

    def arrived_up(m, c, q, p):
        (low, ok, b_end), _ = ends(p)
        straight = p == 0 or is_last(m, c, q)
        pl.when(ok)(lambda: take(m, c, q, low, b_end, has_up, up_dev, up_sem, 0, straight))

    def arrived(m, c, q, p):
        arrived_dn(m, c, q, p)
        arrived_up(m, c, q, p)

    def doubled(c, q, p):
        def take_other(b, more, dev, sem, skip):
            crossed_all(2, b, 4, skip)
            k = tile_of(b, cross, c)
            pl.when(more)(lambda: hop(2, c, k, q, dev, sem, skip, True).start())

        (low, has_low, low_end), (high, has_high, high_end) = ends(p)
        pl.when(jnp.logical_and(has_high, high_end))(
            lambda: take_other(high, has_dn, dn_dev, dn_sem, 1)
        )
        pl.when(jnp.logical_and(has_low, low_end))(
            lambda: take_other(low, has_up, up_dev, up_sem, 0)
        )

    def crossed(m, c, p):
        groups = {n - 1: (m,) if m < 2 else (3, 4), n - 2: () if m < 2 else (2,)}.get(c, ())
        for skip, (b, ok, b_end) in enumerate(ends(p)):
            for g in groups:
                here = jnp.logical_and(ok, jnp.logical_not(b_end)) if g == 4 else ok
                pl.when(here)(lambda b=b, g=g, skip=skip: crossed_all(m, b, g, skip))

    def later(m, c, p, h):
        if c < n - 1:
            return
        for b, ok, _ in ends(p):
            if m == 2:
                downs.append((ok, lambda b=b: down_half(b, h)))
                if h is not y:
                    fins.append((ok, lambda b=b: finish_origin(b)))
            else:
                sums.append((ok, lambda b=b: add_tiles(m, tile_of(b, h, 0), False)))

    def tok_copy(peer, origin):
        return pltpu.make_async_remote_copy(
            src_ref=toks.at[origin], dst_ref=toks.at[origin],
            send_sem=t_sem.at[0], recv_sem=t_sem.at[1],
            device_id=(y, z, peer), device_id_type=MESH,
        )

    plan = [(m, c, q) for m, c in first for q in pieces]
    gain_copy.wait()
    keep(plan[0][0], y, *plan[0][1:])
    for m, c in first[1:]:
        fetch(m, y, c, m * n + c).start()
    tok_fetch.start()
    for m, c in second:
        fetch(m, y, c, 2 * n).start()
    for m, c in first + second:
        fetch(m, cross, c, 2 * n + 1).start()
    pl.semaphore_wait(barrier, has_up.astype(jnp.int32) + has_dn.astype(jnp.int32) + tp)
    tok_all = pltpu.make_async_remote_copy(
        src_ref=toks.at[pl.ds(0, tp - 1)], dst_ref=toks.at[pl.ds(0, tp - 1)],
        send_sem=t_sem.at[0], recv_sem=t_sem.at[1], device_id=y_dev, device_id_type=MESH,
    )
    late = [(m, c, q) for m, c in second for q in pieces]

    def send_own(m, c, q):
        pl.when(has_dn)(lambda: send_dn(m, y, c, q))
        pl.when(has_up)(lambda: send_up(m, y, c, q))

    for before, after in zip(plan, plan[1:]):
        keep(after[0], y, *after[1:])
        send_own(*before)
    tok_fetch.wait()
    wide = own[...].astype(jnp.float32)
    scale = lax.rsqrt(jnp.mean(wide * wide, axis=-1, keepdims=True) + 1e-06)
    send_own(*plan[-1])
    toks[t] = (wide * scale).astype(jnp.bfloat16)
    for m, c, q in late:
        keep(m, y, c, q)
    for peer in peers:
        tok_copy(peer, t).start()
    for m, c, q in plan + late:
        keep(m, cross, c, q)
    order = [(m, cross, c, q) for m, c, q in plan]
    order += [(m, y, c, q) for m, c, q in late]
    order += [(m, cross, c, q) for m, c, q in late]

    @pl.when(z == fs - 1)
    def _():
        for item in order:
            send_dn(*item)

    @pl.when(z == 0)
    def _():
        for item in order:
            send_up(*item)

    waiting = []

    def settle(count):
        while len(waiting) > count:
            m, c, p = waiting.pop(0)
            crossed(m, c, p)
            later(m, c, p, cross)

    for p in range(fs - 1):
        for m, c in first:
            for q in pieces:
                arrived(m, c, q, p)
            later(m, c, p, y)
            waiting.append((m, c, p))
            settle(LAG)
            if p > 0:
                work(sums, 4)
        if p == 0:
            tok_all.wait_recv()
            sums[:0] = [
                (None, lambda m=m, h=h: add_tiles(m, tile_of(z, h, 0), h == 0))
                for m in (0, 1) for h in (0, 1)
            ]

    @pl.when(jnp.logical_not(at_end))
    def _():
        for m, c, q in late:
            send_own(m, c, q)

    for p in range(fs - 2):
        for m, c in second:
            for q in pieces:
                arrived(m, c, q, p)
                if is_last(m, c, q):
                    doubled(c, q, p)
                work(downs, 2)
            if p == 0 and c == 0:
                settle(0)
                work(sums, len(sums))
                hid[...] = (jax.nn.silu(acc_g[...]) * acc_u[...]).astype(jnp.bfloat16)
                pl.when(at_end)(hid_copy.start)
                for h in (0, 1):
                    downs.append((None, lambda h=h: down_half(z, h)))
                fins.append((None, lambda: finish_origin(z)))
            later(m, c, p, y)
            waiting.append((m, c, p))
            settle(1)

    def far_tile(h, c):
        return tile_of(far, h, c)

    far_skip = (far > z).astype(jnp.int32)

    def far_take(c, q):
        k = far_tile(y, c)
        hop(2, c, k, q, y_dev, y_sem, far_skip).wait_recv()
        if not is_last(2, c, q):
            hop(2, c, k, q, y_dev, y_sem, far_skip, True).start()

    for _, c, q in late[:-2]:
        pl.when(at_end)(lambda c=c, q=q: far_take(c, q))
        work(downs, 2)
    settle(0)
    work(downs, len(downs))
    pl.when(at_end)(lambda: far_take(*late[-2][1:]))
    pl.when(by_end)(help_down)
    work(fins, len(fins))
    pl.when(by_end)(help_sum)

    @pl.when(at_end)
    def _():
        far_take(*late[-1][1:])
        for g in (2, 3, 4) if n > 1 else (3, 4):
            crossed_all(2, far, g, far_skip)
        sum_copy.wait_recv()
        for i in range(2 * n):
            mix(far * (2 * n) + i, branch_far[i].astype(jnp.float32))

    def sent(g, count, sem, dev):
        if count:
            rows = (slice(0, cols),) * 3 + (slice(0, middle), slice(middle, cols))
            rows = rows[g]
            ref = full[min(g, 2)].at[pl.ds(0, count), rows]
            pltpu.make_async_remote_copy(
                src_ref=ref, dst_ref=ref, send_sem=sem.at[g], recv_sem=b_sem.at[1],
                device_id=dev, device_id_type=MESH,
            ).wait_send()

    def sends(j, g):
        base = (n, n, n - 1, 1, 1)[g]
        outer = (0, fs - 1)
        twice = lambda b: 2 * base if g == 4 and b in outer else base
        mine = 2 * base if j in outer else base
        up = mine + sum(twice(b) for b in range(j)) if j < fs - 1 else 0
        dn = mine + sum(twice(b) for b in range(j + 1, fs)) if j > 0 else 0
        cross = sum(
            base for b in range(fs)
            if b != j and not (b in outer and (abs(b - j) == 1 or g == 4))
        )
        return up, dn, cross

    for j in range(fs):
        @pl.when(z == j)
        def _(j=j):
            for g in range(5):
                up, dn, cross = sends(j, g)
                sent(g, up, up_sem, up_dev)
                sent(g, dn, dn_sem, dn_dev)
                sent(g, cross, y_sem, y_dev)

    def shared(ref, sem):
        return pltpu.make_async_remote_copy(
            src_ref=ref, dst_ref=ref, send_sem=sem.at[0], recv_sem=b_sem.at[1],
            device_id=y_dev, device_id_type=MESH,
        )

    tok_all.wait_send()
    others = pl.ds(0, (tp - 1) * tok_rows)
    pl.when(at_end)(shared(parts.at[pl.ds(0, tiles - 2 * n), others], ps_sem).wait_send)
    pl.when(jnp.logical_not(at_end))(shared(parts.at[:, others], ps_sem).wait_send)
    pl.when(by_end)(shared(parts_far.at[:, others], p_sem).wait_send)
    pl.when(at_end)(hid_copy.wait_send)
    pl.when(by_end)(sum_copy.wait_send)


def emit_kernel(
    fg, fu, fd, mixed, pg_ref, pb_ref, go_ref, uo_ref, do_ref, res_ref, res, sem, res_sem
):
    tiles = fg.shape[0]
    outs = (go_ref, uo_ref, do_ref)
    for m, src in enumerate((fg, fu, fd)):
        for k in range(tiles):
            at = slice(k * LANES, (k + 1) * LANES)
            pltpu.make_async_copy(src.at[k], outs[m].at[:, at], sem.at[m]).start()
    mix = mixed[...]
    center = jnp.mean(mix, axis=-1, keepdims=True)
    off = mix - center
    spread = jnp.mean(jnp.square(off), axis=-1, keepdims=True)
    res[...] = (
        off * lax.rsqrt(spread + 1e-05) * pg_ref[...] + pb_ref[...]
    ).astype(jnp.bfloat16)
    put = pltpu.make_async_copy(res, res_ref, res_sem)
    put.start()
    for m, out in enumerate(outs):
        pltpu.make_async_copy(out, out, sem.at[m]).wait()
    put.wait()


def fused(fs, tp, n, tokens, gate_master, up_master, down_master, norm_gain, post_gain, post_bias):
    rc, cols = gate_master.shape
    tok_rows, d = tokens.shape
    tiles, rows = d // LANES, tp * tok_rows
    bf, f32 = jnp.bfloat16, jnp.float32
    held = pltpu.VMEM((tiles, cols, LANES), bf)
    vmem = pl.BlockSpec(memory_space=pltpu.VMEM)
    anywhere = pl.BlockSpec(memory_space=pl.ANY)
    dma = pltpu.SemaphoreType.DMA
    sources = (tokens, gate_master.T, up_master.T, down_master.T, norm_gain[None, :])
    kept = pl.pallas_call(
        functools.partial(gather_kernel, fs, tp, n),
        out_shape=(held, held, held, pltpu.VMEM((tok_rows, d), f32)),
        in_specs=[anywhere] * 5,
        out_specs=(vmem,) * 4,
        scratch_shapes=[
            pltpu.VMEM((3, 2 * n, cols, LANES), f32),
            pltpu.VMEM((tok_rows, d), bf),
            pltpu.VMEM((1, d), f32),
            pltpu.VMEM((tp, tok_rows, d), bf),
            pltpu.VMEM((rows, cols), f32),
            pltpu.VMEM((rows, cols), f32),
            pltpu.VMEM((rows, cols), bf),
            pltpu.VMEM((tiles, rows, LANES), bf),
            pltpu.VMEM((tp, tiles, tok_rows, LANES), bf),
            pltpu.VMEM((rows, cols), bf),
            pltpu.VMEM((2 * n, rows, LANES), bf),
            pltpu.VMEM((tp - 1, 2 * n, tok_rows, LANES), bf),
            pltpu.VMEM((2 * n, tok_rows, LANES), bf),
            pltpu.VMEM((2 * n, tok_rows, LANES), bf),
            dma((5,)), dma((5,)), dma((5,)), dma((3 * (fs - 1) * n, 2)), dma((fs - 1, 5)),
            dma((2,)), dma((1,)), dma((fs,)), dma((2 * n + 2,)), dma((2,)),
            dma((2,)), dma((2,)), dma((2,)),
        ],
        compiler_params=pltpu.CompilerParams(
            collective_id=0, has_side_effects=True, vmem_limit_bytes=50 * 2**20
        ),
    )(*(pltpu.with_memory_space_constraint(x, pltpu.HBM) for x in sources))
    ready = jax.ShapeDtypeStruct((cols, d), bf)
    gate, up, down, result = pl.pallas_call(
        emit_kernel,
        out_shape=(ready, ready, ready, jax.ShapeDtypeStruct((tok_rows, d), bf)),
        in_specs=[vmem] * 6,
        out_specs=(anywhere,) * 4,
        scratch_shapes=[
            pltpu.VMEM((tok_rows, d), bf), dma((3,)), pltpu.SemaphoreType.DMA,
        ],
        compiler_params=pltpu.CompilerParams(vmem_limit_bytes=20 * 2**20),
    )(
        *(pltpu.with_memory_space_constraint(x, pltpu.VMEM) for x in kept),
        post_gain[None, :], post_bias[None, :],
    )
    return gate.T, up.T, down.T, result


def solution(mesh):
    grp, fs, tp = mesh.shape["grp"], mesh.shape["fs"], mesh.shape["tp"]

    def local(tokens, gate_master, *rest):
        rc, cols = gate_master.shape
        n = rc // (2 * LANES)
        fits = grp == 2 and fs > 3 and rc % (2 * LANES) == 0 and 2 * n * fs <= 32
        fits = fits and cols % 16 == 0 and tokens.shape[0] % 16 == 0
        fits = fits and cols >= 2 * LANES
        if fits:
            return fused(fs, tp, n, tokens, gate_master, *rest)
        return plain(tokens, gate_master, *rest)

    return jax.shard_map(
        local,
        mesh=mesh,
        in_specs=(
            P(("grp", "fs", "tp"), None),
            P("fs", "tp"),
            P("fs", "tp"),
            P("fs", "tp"),
            P(),
            P(),
            P(),
        ),
        out_specs=(P("grp", "tp"), P("grp", "tp"), P("grp", "tp"), P(("grp", "fs", "tp"), None)),
        check_vma=False,
    )
```

```python
import functools

import jax
import jax.numpy as jnp
from jax import lax
from jax.experimental import pallas as pl
from jax.experimental.pallas import tpu as pltpu
from jax.sharding import PartitionSpec as P

MESH = pl.DeviceIdType.MESH
LANES = 128
LAG = 3


def finish(wide, branch, post_gain, post_bias):
    mixed = jnp.sqrt(jnp.float32(2.0)) * wide + 0.5 * branch
    center = jnp.mean(mixed, axis=-1, keepdims=True)
    spread = jnp.mean(jnp.square(mixed - center), axis=-1, keepdims=True)
    return ((mixed - center) * lax.rsqrt(spread + 1e-05) * post_gain + post_bias).astype(
        jnp.bfloat16
    )


def plain(tokens, gate_master, up_master, down_master, norm_gain, post_gain, post_bias):
    row_count = gate_master.shape[0]
    first_row = lax.axis_index("fs") * row_count
    gain_rows = lax.dynamic_slice_in_dim(norm_gain, first_row, row_count, 0)
    gate_piece = (gain_rows[:, None] * gate_master).astype(jnp.bfloat16)
    up_piece = (gain_rows[:, None] * up_master).astype(jnp.bfloat16)
    down_piece = down_master.astype(jnp.bfloat16)
    gate_ready, up_ready, down_ready = (
        lax.all_gather(gate_piece, "fs", axis=0, tiled=True),
        lax.all_gather(up_piece, "fs", axis=0, tiled=True),
        lax.all_gather(down_piece, "fs", axis=0, tiled=True),
    )
    wide = tokens.astype(jnp.float32)
    normed = (wide * lax.rsqrt(jnp.mean(wide * wide, axis=-1, keepdims=True) + 1e-06)).astype(
        jnp.bfloat16
    )
    piece = lax.all_gather(normed, "tp", axis=0, tiled=True)
    gate = jnp.dot(piece, gate_ready, preferred_element_type=jnp.float32)
    upward = jnp.dot(piece, up_ready, preferred_element_type=jnp.float32)
    hidden = (jax.nn.silu(gate) * upward).astype(jnp.bfloat16)
    branch = lax.psum_scatter(
        lax.dot_general(
            hidden, down_ready, (((1,), (1,)), ((), ())), preferred_element_type=jnp.float32
        ).astype(jnp.bfloat16),
        "tp",
        scatter_dimension=0,
        tiled=True,
    ).astype(jnp.float32)
    result = finish(wide, branch, post_gain, post_bias)
    return (gate_ready, up_ready, down_ready, result)


def gather_kernel(
    fs, tp, n, tok_ref, gm_ref, um_ref, dm_ref, gain_ref,
    fg, fu, fd, mixed,
    stage, own, gain, toks, acc_g, acc_u, hid, parts, got,
    hid_far, parts_far, got_far, sum_far, branch_far,
    up_sem, dn_sem, y_sem, r_sem, x_sem, t_sem, ps_sem, pr_sem, i_sem, l_sem, h_sem, p_sem, b_sem,
):
    y, z, t = lax.axis_index("grp"), lax.axis_index("fs"), lax.axis_index("tp")
    cols, rc = gm_ref.shape
    tok_rows, d = tok_ref.shape
    tiles = d // LANES
    middle = -(-cols // 32) * 16
    pieces = ((0, 0, middle), (1, middle, cols - middle))
    full = (fg, fu, fd)
    masters = (gm_ref, um_ref, dm_ref)
    up_dev = (y, jnp.minimum(z + 1, fs - 1), t)
    dn_dev = (y, jnp.maximum(z - 1, 0), t)
    y_dev = (1 - y, z, t)
    has_up, has_dn = z < fs - 1, z > 0
    at_end = jnp.logical_or(z == 0, z == fs - 1)
    by_end = jnp.logical_or(z == 1, z == fs - 2)
    far = jnp.where(z < 2, fs - 1, 0)
    cross = 1 - y
    end_dev = (y, jnp.where(z == 1, 0, fs - 1), t)
    helper = (y, jnp.where(z == 0, 1, fs - 2), t)
    peers = [lax.rem(t + j, tp) for j in range(1, tp)]
    senders = [lax.rem(t + tp - j, tp) for j in range(1, tp)]
    first = [(m, c) for m in (0, 1) for c in range(n)]
    second = [(2, c) for c in range(n)]

    barrier = pltpu.get_barrier_semaphore()

    def greet(dev):
        pl.semaphore_signal(barrier, inc=1, device_id=dev, device_id_type=MESH)

    pl.when(has_up)(lambda: greet(up_dev))
    pl.when(has_dn)(lambda: greet(dn_dev))
    greet(y_dev)
    for peer in peers:
        greet((y, z, peer))

    def is_last(m, c, q):
        return (m, c, q[0]) == (2, n - 1, 1)

    def group(m, c, q):
        return m if (m, c) != (2, n - 1) else 3 + q[0]

    def fetch(m, h, c, slot):
        k = h * n + c
        return pltpu.make_async_copy(
            masters[m].at[:, pl.ds(pl.multiple_of(k * LANES, LANES), LANES)],
            stage.at[m, k], i_sem.at[slot],
        )

    def fetched(m, h, c):
        if h is not y:
            if (m, c) == first[0]:
                ref = stage.at[:, pl.ds(h * n, n)]
                pltpu.make_async_copy(ref, ref, i_sem.at[2 * n + 1]).wait()
        elif m == 2:
            if c == 0:
                ref = stage.at[2, pl.ds(h * n, n)]
                pltpu.make_async_copy(ref, ref, i_sem.at[2 * n]).wait()
        else:
            fetch(m, h, c, m * n + c).wait()

    gain_copy = pltpu.make_async_copy(gain_ref, gain, l_sem.at[0])
    tok_fetch = pltpu.make_async_copy(tok_ref, own, l_sem.at[1])
    gain_copy.start()
    fetch(first[0][0], y, first[0][1], 0).start()

    def tile_of(b, h, c):
        return b * (2 * n) + h * n + c

    def hop(m, c, k, q, dev, sem, skip, other=False):
        rows = pl.ds(q[1], q[2])
        b = k // (2 * n)
        if other:
            recv_sem = x_sem.at[b - skip, group(m, c, q)]
        else:
            recv_sem = r_sem.at[(m * (fs - 1) + b - skip) * n + c, q[0]]
        return pltpu.make_async_remote_copy(
            src_ref=full[m].at[k, rows], dst_ref=full[m].at[k, rows],
            send_sem=sem.at[group(m, c, q)], recv_sem=recv_sem,
            device_id=dev, device_id_type=MESH,
        )

    def crossed_all(m, b, g, skip):
        k = tile_of(b, cross, 0)
        if g < 3:
            ref = full[m].at[pl.ds(k, (n, n, n - 1)[g])]
        else:
            q = pieces[g - 3]
            ref = full[2].at[k + n - 1, pl.ds(q[1], q[2])]
        pltpu.make_async_remote_copy(
            src_ref=ref, dst_ref=ref, send_sem=y_sem.at[g], recv_sem=x_sem.at[b - skip, g],
            device_id=y_dev, device_id_type=MESH,
        ).wait_recv()

    def keep(m, h, c, q):
        if q[0] == 0:
            fetched(m, h, c)
        k = tile_of(z, h, c)
        rows = pl.ds(q[1], q[2])
        v = stage[m, h * n + c, rows, :]
        if m < 2:
            v = v * gain[:, pl.ds(pl.multiple_of(k * LANES, LANES), LANES)]
        full[m][k, rows, :] = v.astype(jnp.bfloat16)

    def send_up(m, h, c, q):
        hop(m, c, tile_of(z, h, c), q, up_dev, up_sem, 0, h is not y).start()

    def send_dn(m, h, c, q):
        hop(m, c, tile_of(z, h, c), q, dn_dev, dn_sem, 1, h is not y).start()

    def part_copy(b, h, count, j, peer):
        k = tile_of(b, h, 0)
        return pltpu.make_async_remote_copy(
            src_ref=parts.at[
                pl.ds(k, count), pl.ds(pl.multiple_of(peer * tok_rows, tok_rows), tok_rows)
            ],
            dst_ref=got.at[t, pl.ds(k, count)],
            send_sem=ps_sem.at[0], recv_sem=pr_sem.at[b],
            device_id=(y, z, peer), device_id_type=MESH,
        )

    def product(lhs, k, count, to, at):
        rhs = jnp.concatenate([fd[k + i] for i in range(count)], axis=1)
        part = jnp.dot(lhs[...], rhs, preferred_element_type=jnp.float32)
        for i in range(count):
            to[at + i] = part[:, i * LANES:(i + 1) * LANES].astype(jnp.bfloat16)

    def down_half(b, h, count=n):
        k = tile_of(b, h, 0)
        product(hid, k, count, parts, k)
        for j, peer in enumerate(peers):
            part_copy(b, h, count, j, peer).start()

    def add_tiles(m, k, start):
        acc = (acc_g, acc_u)[m]
        at = pl.ds(pl.multiple_of(k * LANES, LANES), n * LANES)
        lhs = toks[:, :, at].reshape(tp * tok_rows, n * LANES)
        rhs = jnp.concatenate([full[m][k + i] for i in range(n)], axis=1)
        term = lax.dot_general(
            lhs, rhs, (((1,), (1,)), ((), ())), preferred_element_type=jnp.float32
        )
        acc[...] = term if start else acc[...] + term

    mine = pl.ds(pl.multiple_of(t * tok_rows, tok_rows), tok_rows)

    def mix(k, branch):
        at = pl.ds(pl.multiple_of(k * LANES, LANES), LANES)
        wide = own[:, at].astype(jnp.float32)
        mixed[:, at] = jnp.sqrt(jnp.float32(2.0)) * wide + 0.5 * branch

    def finish_origin(b, h=0, count=2 * n):
        k = tile_of(b, h, 0)
        ref = got.at[pl.ds(0, tp - 1), pl.ds(k, count)]
        pltpu.make_async_remote_copy(
            src_ref=ref, dst_ref=ref, send_sem=ps_sem.at[0], recv_sem=pr_sem.at[b],
            device_id=y_dev, device_id_type=MESH,
        ).wait_recv()
        for i in range(count):
            branch = parts[k + i, mine, :].astype(jnp.float32)
            for peer in senders:
                branch = branch + got[peer, k + i].astype(jnp.float32)
            mix(k + i, branch)

    hid_copy = pltpu.make_async_remote_copy(
        src_ref=hid, dst_ref=hid_far, send_sem=h_sem.at[0], recv_sem=h_sem.at[1],
        device_id=helper, device_id_type=MESH,
    )
    sum_copy = pltpu.make_async_remote_copy(
        src_ref=sum_far, dst_ref=branch_far, send_sem=b_sem.at[0], recv_sem=b_sem.at[1],
        device_id=end_dev, device_id_type=MESH,
    )

    def far_copy(j, peer):
        return pltpu.make_async_remote_copy(
            src_ref=parts_far.at[
                :, pl.ds(pl.multiple_of(peer * tok_rows, tok_rows), tok_rows)
            ],
            dst_ref=got_far.at[j], send_sem=p_sem.at[0], recv_sem=p_sem.at[1],
            device_id=(y, z, peer), device_id_type=MESH,
        )

    def help_down():
        hid_copy.wait_recv()
        product(hid_far, tile_of(far, cross, 0), n, parts_far, 0)
        product(hid_far, tile_of(far, y, n - 1), 1, parts_far, n)
        for j, peer in enumerate(peers):
            far_copy(j, peer).start()

    def help_sum():
        pltpu.make_async_remote_copy(
            src_ref=got_far, dst_ref=got_far, send_sem=p_sem.at[0], recv_sem=p_sem.at[1],
            device_id=y_dev, device_id_type=MESH,
        ).wait_recv()
        total = parts_far[:, mine, :].astype(jnp.float32)
        for j in range(tp - 1):
            total = total + got_far[j].astype(jnp.float32)
        sum_far[...] = total.astype(jnp.bfloat16)
        sum_copy.start()

    def ends(p):
        low, high = z - 1 - p, z + 1 + p
        return ((low, low >= 0, low == 0), (high, high <= fs - 1, high == fs - 1))

    sums, downs, fins = [], [], []

    def work(todo, count):
        for _ in range(min(count, len(todo))):
            ok, item = todo.pop(0)
            if ok is None:
                item()
            else:
                pl.when(ok)(item)

    def take(m, c, q, b, b_end, more, dev, sem, skip, straight):
        k = tile_of(b, y, c)
        hop(m, c, k, q, dev, sem, skip).wait_recv()
        pl.when(more)(lambda: hop(m, c, k, q, dev, sem, skip).start())
        pass_on = lambda: hop(m, c, k, q, y_dev, y_sem, skip, True).start()
        if straight:
            pl.when(jnp.logical_not(b_end))(pass_on)
        else:
            pass_on()

    def arrived_dn(m, c, q, p):
        _, (high, ok, b_end) = ends(p)
        straight = p == 0 or is_last(m, c, q)
        pl.when(ok)(lambda: take(m, c, q, high, b_end, has_dn, dn_dev, dn_sem, 1, straight))

    def arrived_up(m, c, q, p):
        (low, ok, b_end), _ = ends(p)
        straight = p == 0 or is_last(m, c, q)
        pl.when(ok)(lambda: take(m, c, q, low, b_end, has_up, up_dev, up_sem, 0, straight))

    def arrived(m, c, q, p):
        arrived_dn(m, c, q, p)
        arrived_up(m, c, q, p)

    def doubled(c, q, p):
        def take_other(b, more, dev, sem, skip):
            crossed_all(2, b, 4, skip)
            k = tile_of(b, cross, c)
            pl.when(more)(lambda: hop(2, c, k, q, dev, sem, skip, True).start())

        (low, has_low, low_end), (high, has_high, high_end) = ends(p)
        pl.when(jnp.logical_and(has_high, high_end))(
            lambda: take_other(high, has_dn, dn_dev, dn_sem, 1)
        )
        pl.when(jnp.logical_and(has_low, low_end))(
            lambda: take_other(low, has_up, up_dev, up_sem, 0)
        )

    def crossed(m, c, p):
        groups = {n - 1: (m,) if m < 2 else (3, 4), n - 2: () if m < 2 else (2,)}.get(c, ())
        for skip, (b, ok, b_end) in enumerate(ends(p)):
            for g in groups:
                here = jnp.logical_and(ok, jnp.logical_not(b_end)) if g == 4 else ok
                pl.when(here)(lambda b=b, g=g, skip=skip: crossed_all(m, b, g, skip))

    def later(m, c, p, h):
        if c < n - 1:
            return
        for b, ok, _ in ends(p):
            if m == 2:
                downs.append((ok, lambda b=b: down_half(b, h)))
                if h is not y:
                    fins.append((ok, lambda b=b: finish_origin(b)))
            else:
                sums.append((ok, lambda b=b: add_tiles(m, tile_of(b, h, 0), False)))

    def tok_copy(peer, origin):
        return pltpu.make_async_remote_copy(
            src_ref=toks.at[origin], dst_ref=toks.at[origin],
            send_sem=t_sem.at[0], recv_sem=t_sem.at[1],
            device_id=(y, z, peer), device_id_type=MESH,
        )

    plan = [(m, c, q) for m, c in first for q in pieces]
    gain_copy.wait()
    keep(plan[0][0], y, *plan[0][1:])
    for m, c in first[1:]:
        fetch(m, y, c, m * n + c).start()
    tok_fetch.start()
    for m, c in second:
        fetch(m, y, c, 2 * n).start()
    for m, c in first + second:
        fetch(m, cross, c, 2 * n + 1).start()
    pl.semaphore_wait(barrier, has_up.astype(jnp.int32) + has_dn.astype(jnp.int32) + tp)
    tok_all = pltpu.make_async_remote_copy(
        src_ref=toks.at[pl.ds(0, tp - 1)], dst_ref=toks.at[pl.ds(0, tp - 1)],
        send_sem=t_sem.at[0], recv_sem=t_sem.at[1], device_id=y_dev, device_id_type=MESH,
    )
    late = [(m, c, q) for m, c in second for q in pieces]

    def send_own(m, c, q):
        pl.when(has_dn)(lambda: send_dn(m, y, c, q))
        pl.when(has_up)(lambda: send_up(m, y, c, q))

    for before, after in zip(plan, plan[1:]):
        keep(after[0], y, *after[1:])
        send_own(*before)
    tok_fetch.wait()
    wide = own[...].astype(jnp.float32)
    scale = lax.rsqrt(jnp.mean(wide * wide, axis=-1, keepdims=True) + 1e-06)
    send_own(*plan[-1])
    toks[t] = (wide * scale).astype(jnp.bfloat16)
    for m, c, q in late:
        keep(m, y, c, q)
    for peer in peers:
        tok_copy(peer, t).start()
    for m, c, q in plan + late:
        keep(m, cross, c, q)
    order = [(m, cross, c, q) for m, c, q in plan]
    order += [(m, y, c, q) for m, c, q in late]
    order += [(m, cross, c, q) for m, c, q in late]

    @pl.when(z == fs - 1)
    def _():
        for item in order:
            send_dn(*item)

    @pl.when(z == 0)
    def _():
        for item in order:
            send_up(*item)

    waiting = []

    def settle(count):
        while len(waiting) > count:
            m, c, p = waiting.pop(0)
            crossed(m, c, p)
            later(m, c, p, cross)

    for p in range(fs - 1):
        for m, c in first:
            for q in pieces:
                arrived(m, c, q, p)
            later(m, c, p, y)
            waiting.append((m, c, p))
            settle(LAG)
            if p > 0:
                work(sums, 4)
        if p == 0:
            tok_all.wait_recv()
            sums[:0] = [
                (None, lambda m=m, h=h: add_tiles(m, tile_of(z, h, 0), h == 0))
                for m in (0, 1) for h in (0, 1)
            ]

    @pl.when(jnp.logical_not(at_end))
    def _():
        for m, c, q in late:
            send_own(m, c, q)

    for p in range(fs - 2):
        for m, c in second:
            for q in pieces:
                arrived(m, c, q, p)
                if is_last(m, c, q):
                    doubled(c, q, p)
                work(downs, 2)
            if p == 0 and c == 0:
                settle(0)
                work(sums, len(sums))
                hid[...] = (jax.nn.silu(acc_g[...]) * acc_u[...]).astype(jnp.bfloat16)
                pl.when(at_end)(hid_copy.start)
                for h in (0, 1):
                    downs.append((None, lambda h=h: down_half(z, h)))
                fins.append((None, lambda: finish_origin(z)))
            later(m, c, p, y)
            waiting.append((m, c, p))
            settle(1)

    def far_tile(h, c):
        return tile_of(far, h, c)

    far_skip = (far > z).astype(jnp.int32)

    def far_take(c, q):
        k = far_tile(y, c)
        hop(2, c, k, q, y_dev, y_sem, far_skip).wait_recv()
        if not is_last(2, c, q):
            hop(2, c, k, q, y_dev, y_sem, far_skip, True).start()

    for _, c, q in late[:-2]:
        pl.when(at_end)(lambda c=c, q=q: far_take(c, q))
        work(downs, 2)
    if n > 1:
        downs.append((at_end, lambda: down_half(far, y, n - 1)))
        fins.append((at_end, lambda: finish_origin(far, y, n - 1)))
    settle(0)
    work(downs, len(downs))
    pl.when(at_end)(lambda: far_take(*late[-2][1:]))
    pl.when(by_end)(help_down)
    work(fins, len(fins))
    pl.when(by_end)(help_sum)

    @pl.when(at_end)
    def _():
        far_take(*late[-1][1:])
        for g in (2, 3, 4) if n > 1 else (3, 4):
            crossed_all(2, far, g, far_skip)
        sum_copy.wait_recv()
        for i in range(n):
            mix(far_tile(cross, i), branch_far[i].astype(jnp.float32))
        mix(far_tile(y, n - 1), branch_far[n].astype(jnp.float32))

    def sent(g, count, sem, dev):
        if count:
            rows = (slice(0, cols),) * 3 + (slice(0, middle), slice(middle, cols))
            rows = rows[g]
            ref = full[min(g, 2)].at[pl.ds(0, count), rows]
            pltpu.make_async_remote_copy(
                src_ref=ref, dst_ref=ref, send_sem=sem.at[g], recv_sem=b_sem.at[1],
                device_id=dev, device_id_type=MESH,
            ).wait_send()

    def sends(j, g):
        base = (n, n, n - 1, 1, 1)[g]
        outer = (0, fs - 1)
        twice = lambda b: 2 * base if g == 4 and b in outer else base
        mine = 2 * base if j in outer else base
        up = mine + sum(twice(b) for b in range(j)) if j < fs - 1 else 0
        dn = mine + sum(twice(b) for b in range(j + 1, fs)) if j > 0 else 0
        cross = sum(
            base for b in range(fs)
            if b != j and not (b in outer and (abs(b - j) == 1 or g == 4))
        )
        return up, dn, cross

    for j in range(fs):
        @pl.when(z == j)
        def _(j=j):
            for g in range(5):
                up, dn, cross = sends(j, g)
                sent(g, up, up_sem, up_dev)
                sent(g, dn, dn_sem, dn_dev)
                sent(g, cross, y_sem, y_dev)

    def shared(ref, sem):
        return pltpu.make_async_remote_copy(
            src_ref=ref, dst_ref=ref, send_sem=sem.at[0], recv_sem=b_sem.at[1],
            device_id=y_dev, device_id_type=MESH,
        )

    tok_all.wait_send()
    others = pl.ds(0, (tp - 1) * tok_rows)
    pl.when(at_end)(shared(parts.at[pl.ds(0, tiles - n - 1), others], ps_sem).wait_send)
    pl.when(jnp.logical_not(at_end))(shared(parts.at[:, others], ps_sem).wait_send)
    pl.when(by_end)(shared(parts_far.at[:, others], p_sem).wait_send)
    pl.when(at_end)(hid_copy.wait_send)
    pl.when(by_end)(sum_copy.wait_send)


def emit_kernel(
    fg, fu, fd, mixed, pg_ref, pb_ref, go_ref, uo_ref, do_ref, res_ref, res, sem, res_sem
):
    tiles = fg.shape[0]
    outs = (go_ref, uo_ref, do_ref)
    for m, src in enumerate((fg, fu, fd)):
        for k in range(tiles):
            at = slice(k * LANES, (k + 1) * LANES)
            pltpu.make_async_copy(src.at[k], outs[m].at[:, at], sem.at[m]).start()
    mix = mixed[...]
    center = jnp.mean(mix, axis=-1, keepdims=True)
    off = mix - center
    spread = jnp.mean(jnp.square(off), axis=-1, keepdims=True)
    res[...] = (
        off * lax.rsqrt(spread + 1e-05) * pg_ref[...] + pb_ref[...]
    ).astype(jnp.bfloat16)
    put = pltpu.make_async_copy(res, res_ref, res_sem)
    put.start()
    for m, out in enumerate(outs):
        pltpu.make_async_copy(out, out, sem.at[m]).wait()
    put.wait()


def fused(fs, tp, n, tokens, gate_master, up_master, down_master, norm_gain, post_gain, post_bias):
    rc, cols = gate_master.shape
    tok_rows, d = tokens.shape
    tiles, rows = d // LANES, tp * tok_rows
    bf, f32 = jnp.bfloat16, jnp.float32
    held = pltpu.VMEM((tiles, cols, LANES), bf)
    vmem = pl.BlockSpec(memory_space=pltpu.VMEM)
    anywhere = pl.BlockSpec(memory_space=pl.ANY)
    dma = pltpu.SemaphoreType.DMA
    sources = (tokens, gate_master.T, up_master.T, down_master.T, norm_gain[None, :])
    kept = pl.pallas_call(
        functools.partial(gather_kernel, fs, tp, n),
        out_shape=(held, held, held, pltpu.VMEM((tok_rows, d), f32)),
        in_specs=[anywhere] * 5,
        out_specs=(vmem,) * 4,
        scratch_shapes=[
            pltpu.VMEM((3, 2 * n, cols, LANES), f32),
            pltpu.VMEM((tok_rows, d), bf),
            pltpu.VMEM((1, d), f32),
            pltpu.VMEM((tp, tok_rows, d), bf),
            pltpu.VMEM((rows, cols), f32),
            pltpu.VMEM((rows, cols), f32),
            pltpu.VMEM((rows, cols), bf),
            pltpu.VMEM((tiles, rows, LANES), bf),
            pltpu.VMEM((tp, tiles, tok_rows, LANES), bf),
            pltpu.VMEM((rows, cols), bf),
            pltpu.VMEM((n + 1, rows, LANES), bf),
            pltpu.VMEM((tp - 1, n + 1, tok_rows, LANES), bf),
            pltpu.VMEM((n + 1, tok_rows, LANES), bf),
            pltpu.VMEM((n + 1, tok_rows, LANES), bf),
            dma((5,)), dma((5,)), dma((5,)), dma((3 * (fs - 1) * n, 2)), dma((fs - 1, 5)),
            dma((2,)), dma((1,)), dma((fs,)), dma((2 * n + 2,)), dma((2,)),
            dma((2,)), dma((2,)), dma((2,)),
        ],
        compiler_params=pltpu.CompilerParams(
            collective_id=0, has_side_effects=True, vmem_limit_bytes=50 * 2**20
        ),
    )(*(pltpu.with_memory_space_constraint(x, pltpu.HBM) for x in sources))
    ready = jax.ShapeDtypeStruct((cols, d), bf)
    gate, up, down, result = pl.pallas_call(
        emit_kernel,
        out_shape=(ready, ready, ready, jax.ShapeDtypeStruct((tok_rows, d), bf)),
        in_specs=[vmem] * 6,
        out_specs=(anywhere,) * 4,
        scratch_shapes=[
            pltpu.VMEM((tok_rows, d), bf), dma((3,)), pltpu.SemaphoreType.DMA,
        ],
        compiler_params=pltpu.CompilerParams(vmem_limit_bytes=20 * 2**20),
    )(
        *(pltpu.with_memory_space_constraint(x, pltpu.VMEM) for x in kept),
        post_gain[None, :], post_bias[None, :],
    )
    return gate.T, up.T, down.T, result


def solution(mesh):
    grp, fs, tp = mesh.shape["grp"], mesh.shape["fs"], mesh.shape["tp"]

    def local(tokens, gate_master, *rest):
        rc, cols = gate_master.shape
        n = rc // (2 * LANES)
        fits = grp == 2 and fs > 3 and rc % (2 * LANES) == 0 and 2 * n * fs <= 32
        fits = fits and cols % 16 == 0 and tokens.shape[0] % 16 == 0
        fits = fits and cols >= 2 * LANES
        if fits:
            return fused(fs, tp, n, tokens, gate_master, *rest)
        return plain(tokens, gate_master, *rest)

    return jax.shard_map(
        local,
        mesh=mesh,
        in_specs=(
            P(("grp", "fs", "tp"), None),
            P("fs", "tp"),
            P("fs", "tp"),
            P("fs", "tp"),
            P(),
            P(),
            P(),
        ),
        out_specs=(P("grp", "tp"), P("grp", "tp"), P("grp", "tp"), P(("grp", "fs", "tp"), None)),
        check_vma=False,
    )
```

```python
import functools

import jax
import jax.numpy as jnp
from jax import lax
from jax.experimental import pallas as pl
from jax.experimental.pallas import tpu as pltpu
from jax.sharding import PartitionSpec as P

MESH = pl.DeviceIdType.MESH
LANES = 128
LAG = 3


def finish(wide, branch, post_gain, post_bias):
    mixed = jnp.sqrt(jnp.float32(2.0)) * wide + 0.5 * branch
    center = jnp.mean(mixed, axis=-1, keepdims=True)
    spread = jnp.mean(jnp.square(mixed - center), axis=-1, keepdims=True)
    return ((mixed - center) * lax.rsqrt(spread + 1e-05) * post_gain + post_bias).astype(
        jnp.bfloat16
    )


def plain(tokens, gate_master, up_master, down_master, norm_gain, post_gain, post_bias):
    row_count = gate_master.shape[0]
    first_row = lax.axis_index("fs") * row_count
    gain_rows = lax.dynamic_slice_in_dim(norm_gain, first_row, row_count, 0)
    gate_piece = (gain_rows[:, None] * gate_master).astype(jnp.bfloat16)
    up_piece = (gain_rows[:, None] * up_master).astype(jnp.bfloat16)
    down_piece = down_master.astype(jnp.bfloat16)
    gate_ready, up_ready, down_ready = (
        lax.all_gather(gate_piece, "fs", axis=0, tiled=True),
        lax.all_gather(up_piece, "fs", axis=0, tiled=True),
        lax.all_gather(down_piece, "fs", axis=0, tiled=True),
    )
    wide = tokens.astype(jnp.float32)
    normed = (wide * lax.rsqrt(jnp.mean(wide * wide, axis=-1, keepdims=True) + 1e-06)).astype(
        jnp.bfloat16
    )
    piece = lax.all_gather(normed, "tp", axis=0, tiled=True)
    gate = jnp.dot(piece, gate_ready, preferred_element_type=jnp.float32)
    upward = jnp.dot(piece, up_ready, preferred_element_type=jnp.float32)
    hidden = (jax.nn.silu(gate) * upward).astype(jnp.bfloat16)
    branch = lax.psum_scatter(
        lax.dot_general(
            hidden, down_ready, (((1,), (1,)), ((), ())), preferred_element_type=jnp.float32
        ).astype(jnp.bfloat16),
        "tp",
        scatter_dimension=0,
        tiled=True,
    ).astype(jnp.float32)
    result = finish(wide, branch, post_gain, post_bias)
    return (gate_ready, up_ready, down_ready, result)


def gather_kernel(
    fs, tp, n, tok_ref, gm_ref, um_ref, dm_ref, gain_ref,
    fg, fu, fd, mixed,
    stage, own, gain, toks, acc_g, acc_u, hid, parts, got,
    hid_far, parts_far, got_far, sum_far, branch_far,
    up_sem, dn_sem, y_sem, r_sem, x_sem, t_sem, ps_sem, pr_sem, i_sem, l_sem, p_sem, b_sem,
):
    y, z, t = lax.axis_index("grp"), lax.axis_index("fs"), lax.axis_index("tp")
    cols, rc = gm_ref.shape
    tok_rows, d = tok_ref.shape
    tiles = d // LANES
    middle = -(-cols // 32) * 16
    pieces = ((0, 0, middle), (1, middle, cols - middle))
    full = (fg, fu, fd)
    masters = (gm_ref, um_ref, dm_ref)
    up_dev = (y, jnp.minimum(z + 1, fs - 1), t)
    dn_dev = (y, jnp.maximum(z - 1, 0), t)
    y_dev = (1 - y, z, t)
    has_up, has_dn = z < fs - 1, z > 0
    at_end = jnp.logical_or(z == 0, z == fs - 1)
    by_end = jnp.logical_or(z == 1, z == fs - 2)
    far = jnp.where(z < 2, fs - 1, 0)
    cross = 1 - y
    end_dev = (y, jnp.where(z == 1, 0, fs - 1), t)
    helper = (y, jnp.where(z == 0, 1, fs - 2), t)
    peers = [lax.rem(t + j, tp) for j in range(1, tp)]
    senders = [lax.rem(t + tp - j, tp) for j in range(1, tp)]
    first = [(m, c) for m in (0, 1) for c in range(n)]
    second = [(2, c) for c in range(n)]

    barrier = pltpu.get_barrier_semaphore()

    def greet(dev):
        pl.semaphore_signal(barrier, inc=1, device_id=dev, device_id_type=MESH)

    pl.when(has_up)(lambda: greet(up_dev))
    pl.when(has_dn)(lambda: greet(dn_dev))
    greet(y_dev)
    for peer in peers:
        greet((y, z, peer))

    def is_last(m, c, q):
        return (m, c, q[0]) == (2, n - 1, 1)

    def group(m, c, q):
        return max(m - 1, 0) if (m, c) != (2, n - 1) else 2 + q[0]

    def fetch(m, h, c, slot):
        k = h * n + c
        return pltpu.make_async_copy(
            masters[m].at[:, pl.ds(pl.multiple_of(k * LANES, LANES), LANES)],
            stage.at[m, k], i_sem.at[slot],
        )

    def fetched(m, h, c):
        if h is not y:
            if (m, c) == first[0]:
                ref = stage.at[:, pl.ds(h * n, n)]
                pltpu.make_async_copy(ref, ref, i_sem.at[2 * n + 1]).wait()
        elif m == 2:
            if c == 0:
                ref = stage.at[2, pl.ds(h * n, n)]
                pltpu.make_async_copy(ref, ref, i_sem.at[2 * n]).wait()
        else:
            fetch(m, h, c, m * n + c).wait()

    gain_copy = pltpu.make_async_copy(gain_ref, gain, l_sem.at[0])
    tok_fetch = pltpu.make_async_copy(tok_ref, own, l_sem.at[1])
    gain_copy.start()
    fetch(first[0][0], y, first[0][1], 0).start()

    def tile_of(b, h, c):
        return b * (2 * n) + h * n + c

    def hop(m, c, k, q, dev, sem, skip, other=False):
        rows = pl.ds(q[1], q[2])
        b = k // (2 * n)
        if other:
            recv_sem = x_sem.at[b - skip, group(m, c, q)]
        else:
            recv_sem = r_sem.at[(m * (fs - 1) + b - skip) * n + c, q[0]]
        return pltpu.make_async_remote_copy(
            src_ref=full[m].at[k, rows], dst_ref=full[m].at[k, rows],
            send_sem=sem.at[group(m, c, q)], recv_sem=recv_sem,
            device_id=dev, device_id_type=MESH,
        )

    def crossed_all(b, g, skip):
        k = tile_of(b, cross, 0)
        if g == 0:
            ref = full[0].at[pl.ds(tile_of(b, 0, 0), 2 * n)]
        elif g == 1:
            ref = full[2].at[pl.ds(k, n - 1)]
        else:
            q = pieces[g - 2]
            ref = full[2].at[k + n - 1, pl.ds(q[1], q[2])]
        pltpu.make_async_remote_copy(
            src_ref=ref, dst_ref=ref, send_sem=y_sem.at[g], recv_sem=x_sem.at[b - skip, g],
            device_id=y_dev, device_id_type=MESH,
        ).wait_recv()

    def keep(m, h, c, q):
        if q[0] == 0:
            fetched(m, h, c)
        k = tile_of(z, h, c)
        rows = pl.ds(q[1], q[2])
        v = stage[m, h * n + c, rows, :]
        if m < 2:
            v = v * gain[:, pl.ds(pl.multiple_of(k * LANES, LANES), LANES)]
        full[m][k, rows, :] = v.astype(jnp.bfloat16)

    def send_up(m, h, c, q):
        hop(m, c, tile_of(z, h, c), q, up_dev, up_sem, 0, h is not y).start()

    def send_dn(m, h, c, q):
        hop(m, c, tile_of(z, h, c), q, dn_dev, dn_sem, 1, h is not y).start()

    def part_copy(b, h, count, j, peer):
        k = tile_of(b, h, 0)
        return pltpu.make_async_remote_copy(
            src_ref=parts.at[
                pl.ds(k, count), pl.ds(pl.multiple_of(peer * tok_rows, tok_rows), tok_rows)
            ],
            dst_ref=got.at[t, pl.ds(k, count)],
            send_sem=ps_sem.at[0], recv_sem=pr_sem.at[b],
            device_id=(y, z, peer), device_id_type=MESH,
        )

    def product(lhs, k, count, to, at):
        rhs = jnp.concatenate([fd[k + i] for i in range(count)], axis=1)
        part = jnp.dot(lhs[...], rhs, preferred_element_type=jnp.float32)
        for i in range(count):
            to[at + i] = part[:, i * LANES:(i + 1) * LANES].astype(jnp.bfloat16)

    def down_half(b, h, count=n):
        k = tile_of(b, h, 0)
        product(hid, k, count, parts, k)
        for j, peer in enumerate(peers):
            part_copy(b, h, count, j, peer).start()

    def add_tiles(m, k, start):
        acc = (acc_g, acc_u)[m]
        at = pl.ds(pl.multiple_of(k * LANES, LANES), n * LANES)
        lhs = toks[:, :, at].reshape(tp * tok_rows, n * LANES)
        rhs = jnp.concatenate([full[m][k + i] for i in range(n)], axis=1)
        term = lax.dot_general(
            lhs, rhs, (((1,), (1,)), ((), ())), preferred_element_type=jnp.float32
        )
        acc[...] = term if start else acc[...] + term

    mine = pl.ds(pl.multiple_of(t * tok_rows, tok_rows), tok_rows)

    def mix(k, branch):
        at = pl.ds(pl.multiple_of(k * LANES, LANES), LANES)
        wide = own[:, at].astype(jnp.float32)
        mixed[:, at] = jnp.sqrt(jnp.float32(2.0)) * wide + 0.5 * branch

    def finish_origin(b, h=0, count=2 * n):
        k = tile_of(b, h, 0)
        ref = got.at[pl.ds(0, tp - 1), pl.ds(k, count)]
        pltpu.make_async_remote_copy(
            src_ref=ref, dst_ref=ref, send_sem=ps_sem.at[0], recv_sem=pr_sem.at[b],
            device_id=y_dev, device_id_type=MESH,
        ).wait_recv()
        for i in range(count):
            branch = parts[k + i, mine, :].astype(jnp.float32)
            for peer in senders:
                branch = branch + got[peer, k + i].astype(jnp.float32)
            mix(k + i, branch)

    hid_copy = pltpu.make_async_remote_copy(
        src_ref=hid, dst_ref=hid_far, send_sem=b_sem.at[0], recv_sem=b_sem.at[1],
        device_id=helper, device_id_type=MESH,
    )
    sum_copy = pltpu.make_async_remote_copy(
        src_ref=sum_far, dst_ref=branch_far, send_sem=b_sem.at[0], recv_sem=b_sem.at[1],
        device_id=end_dev, device_id_type=MESH,
    )

    def far_copy(j, peer):
        return pltpu.make_async_remote_copy(
            src_ref=parts_far.at[
                :, pl.ds(pl.multiple_of(peer * tok_rows, tok_rows), tok_rows)
            ],
            dst_ref=got_far.at[j], send_sem=p_sem.at[0], recv_sem=p_sem.at[1],
            device_id=(y, z, peer), device_id_type=MESH,
        )

    def help_down():
        hid_copy.wait_recv()
        product(hid_far, tile_of(far, cross, 0), n, parts_far, 0)
        product(hid_far, tile_of(far, y, n - 1), 1, parts_far, n)
        for j, peer in enumerate(peers):
            far_copy(j, peer).start()

    def help_sum():
        pltpu.make_async_remote_copy(
            src_ref=got_far, dst_ref=got_far, send_sem=p_sem.at[0], recv_sem=p_sem.at[1],
            device_id=y_dev, device_id_type=MESH,
        ).wait_recv()
        total = parts_far[:, mine, :].astype(jnp.float32)
        for j in range(tp - 1):
            total = total + got_far[j].astype(jnp.float32)
        sum_far[...] = total.astype(jnp.bfloat16)
        sum_copy.start()

    def ends(p):
        low, high = z - 1 - p, z + 1 + p
        return ((low, low >= 0, low == 0), (high, high <= fs - 1, high == fs - 1))

    sums, downs, fins = [], [], []

    def work(todo, count):
        for _ in range(min(count, len(todo))):
            ok, item = todo.pop(0)
            if ok is None:
                item()
            else:
                pl.when(ok)(item)

    def take(m, c, q, b, b_end, more, dev, sem, skip, straight):
        k = tile_of(b, y, c)
        hop(m, c, k, q, dev, sem, skip).wait_recv()
        pl.when(more)(lambda: hop(m, c, k, q, dev, sem, skip).start())
        pass_on = lambda: hop(m, c, k, q, y_dev, y_sem, skip, True).start()
        if straight:
            pl.when(jnp.logical_not(b_end))(pass_on)
        else:
            pass_on()

    def arrived_dn(m, c, q, p):
        _, (high, ok, b_end) = ends(p)
        straight = p == 0 or is_last(m, c, q)
        pl.when(ok)(lambda: take(m, c, q, high, b_end, has_dn, dn_dev, dn_sem, 1, straight))

    def arrived_up(m, c, q, p):
        (low, ok, b_end), _ = ends(p)
        straight = p == 0 or is_last(m, c, q)
        pl.when(ok)(lambda: take(m, c, q, low, b_end, has_up, up_dev, up_sem, 0, straight))

    def arrived(m, c, q, p):
        arrived_dn(m, c, q, p)
        arrived_up(m, c, q, p)

    def doubled(c, q, p):
        def take_other(b, more, dev, sem, skip):
            crossed_all(b, 3, skip)
            k = tile_of(b, cross, c)
            pl.when(more)(lambda: hop(2, c, k, q, dev, sem, skip, True).start())

        (low, has_low, low_end), (high, has_high, high_end) = ends(p)
        pl.when(jnp.logical_and(has_high, high_end))(
            lambda: take_other(high, has_dn, dn_dev, dn_sem, 1)
        )
        pl.when(jnp.logical_and(has_low, low_end))(
            lambda: take_other(low, has_up, up_dev, up_sem, 0)
        )

    def crossed(m, c, p):
        groups = {(1, n - 1): (0,), (2, n - 1): (2, 3), (2, n - 2): (1,)}.get((m, c), ())
        for skip, (b, ok, b_end) in enumerate(ends(p)):
            for g in groups:
                here = jnp.logical_and(ok, jnp.logical_not(b_end)) if g == 3 else ok
                pl.when(here)(lambda b=b, g=g, skip=skip: crossed_all(b, g, skip))

    def later(m, c, p, h):
        if c < n - 1:
            return
        for b, ok, _ in ends(p):
            if m == 2:
                downs.append((ok, lambda b=b: down_half(b, h)))
                if h is not y:
                    fins.append((ok, lambda b=b: finish_origin(b)))
            else:
                for w in (m,) if h is y else (0, 1) if m == 1 else ():
                    sums.append((ok, lambda b=b, w=w: add_tiles(w, tile_of(b, h, 0), False)))

    def tok_copy(peer, origin):
        return pltpu.make_async_remote_copy(
            src_ref=toks.at[origin], dst_ref=toks.at[origin],
            send_sem=t_sem.at[0], recv_sem=t_sem.at[1],
            device_id=(y, z, peer), device_id_type=MESH,
        )

    plan = [(m, c, q) for m, c in first for q in pieces]
    gain_copy.wait()
    keep(plan[0][0], y, *plan[0][1:])
    for m, c in first[1:]:
        fetch(m, y, c, m * n + c).start()
    tok_fetch.start()
    for m, c in second:
        fetch(m, y, c, 2 * n).start()
    for m, c in first + second:
        fetch(m, cross, c, 2 * n + 1).start()
    pl.semaphore_wait(barrier, has_up.astype(jnp.int32) + has_dn.astype(jnp.int32) + tp)
    tok_all = pltpu.make_async_remote_copy(
        src_ref=toks.at[pl.ds(0, tp - 1)], dst_ref=toks.at[pl.ds(0, tp - 1)],
        send_sem=t_sem.at[0], recv_sem=t_sem.at[1], device_id=y_dev, device_id_type=MESH,
    )
    late = [(m, c, q) for m, c in second for q in pieces]

    def send_own(m, c, q):
        pl.when(has_dn)(lambda: send_dn(m, y, c, q))
        pl.when(has_up)(lambda: send_up(m, y, c, q))

    for before, after in zip(plan, plan[1:]):
        keep(after[0], y, *after[1:])
        send_own(*before)
    tok_fetch.wait()
    wide = own[...].astype(jnp.float32)
    scale = lax.rsqrt(jnp.mean(wide * wide, axis=-1, keepdims=True) + 1e-06)
    send_own(*plan[-1])
    toks[t] = (wide * scale).astype(jnp.bfloat16)
    for m, c, q in late:
        keep(m, y, c, q)
    for peer in peers:
        tok_copy(peer, t).start()
    for m, c, q in plan + late:
        keep(m, cross, c, q)
    order = [(m, cross, c, q) for m, c, q in plan]
    order += [(m, y, c, q) for m, c, q in late]
    order += [(m, cross, c, q) for m, c, q in late]

    @pl.when(z == fs - 1)
    def _():
        for item in order:
            send_dn(*item)

    @pl.when(z == 0)
    def _():
        for item in order:
            send_up(*item)

    waiting = []

    def settle(count):
        while len(waiting) > count:
            m, c, p = waiting.pop(0)
            crossed(m, c, p)
            later(m, c, p, cross)

    for p in range(fs - 1):
        for m, c in first:
            for q in pieces:
                arrived(m, c, q, p)
            later(m, c, p, y)
            waiting.append((m, c, p))
            settle(LAG)
            if p > 0:
                work(sums, 4)
        if p == 0:
            tok_all.wait_recv()
            sums[:0] = [
                (None, lambda m=m, h=h: add_tiles(m, tile_of(z, h, 0), h == 0))
                for m in (0, 1) for h in (0, 1)
            ]

    @pl.when(jnp.logical_not(at_end))
    def _():
        for m, c, q in late:
            send_own(m, c, q)

    for p in range(fs - 2):
        for m, c in second:
            for q in pieces:
                arrived(m, c, q, p)
                if is_last(m, c, q):
                    doubled(c, q, p)
                work(downs, 2)
            if p == 0 and c == 0:
                settle(0)
                work(sums, len(sums))
                hid[...] = (jax.nn.silu(acc_g[...]) * acc_u[...]).astype(jnp.bfloat16)
                pl.when(at_end)(hid_copy.start)
                for h in (0, 1):
                    downs.append((None, lambda h=h: down_half(z, h)))
                fins.append((None, lambda: finish_origin(z)))
            later(m, c, p, y)
            waiting.append((m, c, p))
            settle(1)

    def far_tile(h, c):
        return tile_of(far, h, c)

    far_skip = (far > z).astype(jnp.int32)

    def far_take(c, q):
        k = far_tile(y, c)
        hop(2, c, k, q, y_dev, y_sem, far_skip).wait_recv()
        if not is_last(2, c, q):
            hop(2, c, k, q, y_dev, y_sem, far_skip, True).start()

    for _, c, q in late[:-2]:
        pl.when(at_end)(lambda c=c, q=q: far_take(c, q))
        work(downs, 2)
    if n > 1:
        downs.append((at_end, lambda: down_half(far, y, n - 1)))
        fins.append((at_end, lambda: finish_origin(far, y, n - 1)))
    settle(0)
    work(downs, len(downs))
    pl.when(at_end)(lambda: far_take(*late[-2][1:]))
    pl.when(by_end)(help_down)
    work(fins, len(fins))
    pl.when(by_end)(help_sum)

    @pl.when(at_end)
    def _():
        far_take(*late[-1][1:])
        for g in (1, 2, 3) if n > 1 else (2, 3):
            crossed_all(far, g, far_skip)
        sum_copy.wait_recv()
        for i in range(n):
            mix(far_tile(cross, i), branch_far[i].astype(jnp.float32))
        mix(far_tile(y, n - 1), branch_far[n].astype(jnp.float32))

    def sent(g, count, sem, dev):
        if count:
            rows = (slice(0, cols),) * 2 + (slice(0, middle), slice(middle, cols))
            rows = rows[g]
            ref = full[2 if g else 0].at[pl.ds(0, count), rows]
            pltpu.make_async_remote_copy(
                src_ref=ref, dst_ref=ref, send_sem=sem.at[g], recv_sem=b_sem.at[1],
                device_id=dev, device_id_type=MESH,
            ).wait_send()

    def sends(j, g):
        base = (2 * n, n - 1, 1, 1)[g]
        outer = (0, fs - 1)
        twice = lambda b: 2 * base if g == 3 and b in outer else base
        mine = 2 * base if j in outer else base
        up = mine + sum(twice(b) for b in range(j)) if j < fs - 1 else 0
        dn = mine + sum(twice(b) for b in range(j + 1, fs)) if j > 0 else 0
        cross = sum(
            base for b in range(fs)
            if b != j and not (b in outer and (abs(b - j) == 1 or g == 3))
        )
        return up, dn, cross

    for j in range(fs):
        @pl.when(z == j)
        def _(j=j):
            for g in range(4):
                up, dn, cross = sends(j, g)
                sent(g, up, up_sem, up_dev)
                sent(g, dn, dn_sem, dn_dev)
                sent(g, cross, y_sem, y_dev)

    def shared(ref, sem):
        return pltpu.make_async_remote_copy(
            src_ref=ref, dst_ref=ref, send_sem=sem.at[0], recv_sem=b_sem.at[1],
            device_id=y_dev, device_id_type=MESH,
        )

    tok_all.wait_send()
    others = pl.ds(0, (tp - 1) * tok_rows)
    pl.when(at_end)(shared(parts.at[pl.ds(0, tiles - n - 1), others], ps_sem).wait_send)
    pl.when(jnp.logical_not(at_end))(shared(parts.at[:, others], ps_sem).wait_send)
    pl.when(by_end)(shared(parts_far.at[:, others], p_sem).wait_send)
    pl.when(at_end)(hid_copy.wait_send)
    pl.when(by_end)(sum_copy.wait_send)


def emit_kernel(
    fg, fu, fd, mixed, pg_ref, pb_ref, go_ref, uo_ref, do_ref, res_ref, res, sem, res_sem
):
    tiles = fg.shape[0]
    outs = (go_ref, uo_ref, do_ref)
    for m, src in enumerate((fg, fu, fd)):
        for k in range(tiles):
            at = slice(k * LANES, (k + 1) * LANES)
            pltpu.make_async_copy(src.at[k], outs[m].at[:, at], sem.at[m]).start()
    mix = mixed[...]
    center = jnp.mean(mix, axis=-1, keepdims=True)
    off = mix - center
    spread = jnp.mean(jnp.square(off), axis=-1, keepdims=True)
    res[...] = (
        off * lax.rsqrt(spread + 1e-05) * pg_ref[...] + pb_ref[...]
    ).astype(jnp.bfloat16)
    put = pltpu.make_async_copy(res, res_ref, res_sem)
    put.start()
    for m, out in enumerate(outs):
        pltpu.make_async_copy(out, out, sem.at[m]).wait()
    put.wait()


def fused(fs, tp, n, tokens, gate_master, up_master, down_master, norm_gain, post_gain, post_bias):
    rc, cols = gate_master.shape
    tok_rows, d = tokens.shape
    tiles, rows = d // LANES, tp * tok_rows
    bf, f32 = jnp.bfloat16, jnp.float32
    held = pltpu.VMEM((tiles, cols, LANES), bf)
    vmem = pl.BlockSpec(memory_space=pltpu.VMEM)
    anywhere = pl.BlockSpec(memory_space=pl.ANY)
    dma = pltpu.SemaphoreType.DMA
    sources = (tokens, gate_master.T, up_master.T, down_master.T, norm_gain[None, :])
    kept = pl.pallas_call(
        functools.partial(gather_kernel, fs, tp, n),
        out_shape=(held, held, held, pltpu.VMEM((tok_rows, d), f32)),
        in_specs=[anywhere] * 5,
        out_specs=(vmem,) * 4,
        scratch_shapes=[
            pltpu.VMEM((3, 2 * n, cols, LANES), f32),
            pltpu.VMEM((tok_rows, d), bf),
            pltpu.VMEM((1, d), f32),
            pltpu.VMEM((tp, tok_rows, d), bf),
            pltpu.VMEM((rows, cols), f32),
            pltpu.VMEM((rows, cols), f32),
            pltpu.VMEM((rows, cols), bf),
            pltpu.VMEM((tiles, rows, LANES), bf),
            pltpu.VMEM((tp, tiles, tok_rows, LANES), bf),
            pltpu.VMEM((rows, cols), bf),
            pltpu.VMEM((n + 1, rows, LANES), bf),
            pltpu.VMEM((tp - 1, n + 1, tok_rows, LANES), bf),
            pltpu.VMEM((n + 1, tok_rows, LANES), bf),
            pltpu.VMEM((n + 1, tok_rows, LANES), bf),
            dma((4,)), dma((4,)), dma((4,)), dma((3 * (fs - 1) * n, 2)), dma((fs - 1, 4)),
            dma((2,)), dma((1,)), dma((fs,)), dma((2 * n + 2,)), dma((2,)),
            dma((2,)), dma((2,)),
        ],
        compiler_params=pltpu.CompilerParams(
            collective_id=0, has_side_effects=True, vmem_limit_bytes=50 * 2**20
        ),
    )(*(pltpu.with_memory_space_constraint(x, pltpu.HBM) for x in sources))
    ready = jax.ShapeDtypeStruct((cols, d), bf)
    gate, up, down, result = pl.pallas_call(
        emit_kernel,
        out_shape=(ready, ready, ready, jax.ShapeDtypeStruct((tok_rows, d), bf)),
        in_specs=[vmem] * 6,
        out_specs=(anywhere,) * 4,
        scratch_shapes=[
            pltpu.VMEM((tok_rows, d), bf), dma((3,)), pltpu.SemaphoreType.DMA,
        ],
        compiler_params=pltpu.CompilerParams(vmem_limit_bytes=20 * 2**20),
    )(
        *(pltpu.with_memory_space_constraint(x, pltpu.VMEM) for x in kept),
        post_gain[None, :], post_bias[None, :],
    )
    return gate.T, up.T, down.T, result


def solution(mesh):
    grp, fs, tp = mesh.shape["grp"], mesh.shape["fs"], mesh.shape["tp"]

    def local(tokens, gate_master, *rest):
        rc, cols = gate_master.shape
        n = rc // (2 * LANES)
        fits = grp == 2 and fs > 3 and rc % (2 * LANES) == 0 and 2 * n * fs <= 32
        fits = fits and cols % 16 == 0 and tokens.shape[0] % 16 == 0
        fits = fits and cols >= 2 * LANES
        if fits:
            return fused(fs, tp, n, tokens, gate_master, *rest)
        return plain(tokens, gate_master, *rest)

    return jax.shard_map(
        local,
        mesh=mesh,
        in_specs=(
            P(("grp", "fs", "tp"), None),
            P("fs", "tp"),
            P("fs", "tp"),
            P("fs", "tp"),
            P(),
            P(),
            P(),
        ),
        out_specs=(P("grp", "tp"), P("grp", "tp"), P("grp", "tp"), P(("grp", "fs", "tp"), None)),
        check_vma=False,
    )
```
